32 devices in a mesh: sp: 8 (over z, y), tp: 4 (over x, core).
Axes of the slice: x: 2, y: 2, z: 4, core: 2. Of those that a mesh axis runs over, the one named last changes fastest.
Arguments:
- arriving_hidden_sum: bfloat16 [8192, 2048], P('sp'), may hold values from -40 to 40
- content_entries_clustered: bfloat16 [8192, 4096], P('sp', 'tp'), may hold values from -6 to 6
- leaving_switch_entries: bfloat16 [8192, 4096], P('sp', 'tp'), may hold values from -6 to 6
- linked_source_target_pairs: bfloat16 [8192, 8, 2, 128], P('sp', 'tp'), may hold values from -1.78125 to 1.78125
- raw_interval_length: bfloat16 [8192, 64], P('sp', 'tp'), may hold values from -5 to 5
- spike_extra_lognoise: float32 [8192, 64], P('sp', 'tp'), may hold values from -0.6 to 0
- content_filter_kernel: bfloat16 [4, 4096], P(None, 'tp'), may hold values from -3 to 3
- coupling_filter_kernel: bfloat16 [4, 8, 2, 128], P(None, 'tp'), may hold values from -3 to 3
- interval_shift_vector: float32 [64], P('tp'), may hold values from -0.5 to 0.5
- fading_speed_exponent: float32 [64], P('tp'), may hold values from -16 to -2.9
- skip_channel_factor: float32 [64], P('tp'), may hold values from 1 to 10
- cluster_rescale_vector: float32 [4096], P('tp'), may hold values from 0.1 to 1.9
- blender_final_tensor: bfloat16 [4096, 2048], P('tp'), may hold values from -0.09375 to 0.09375
- prelayer_rescale_vector: float32 [2048], replicated, may hold values from 0.1 to 1.9
- switching_linear_tensor: bfloat16 [2048, 5632], P('sp', 'tp'), may hold values from -0.125 to 0.125
- widening_linear_tensor: bfloat16 [2048, 5632], P('sp', 'tp'), may hold values from -0.125 to 0.125
- contracting_linear_tensor: bfloat16 [5632, 2048], P('tp', 'sp'), may hold values from -0.078125 to 0.078125
Outputs:
- residual_out: bfloat16 [8192, 2048], P('sp', 'tp')
The draws below stay inside these ranges and needn't reach their ends.
All inputs are finite; a program needn't handle non-finite values.
Results may differ from the reference program's by a relative error of at most 0.012.
Values may be sent and summed in bfloat16 or wider, within the bound.
A program may use at most 128 MiB of HBM per device.

```python
import math
import jax
import jax.numpy as jnp
from jax import lax

D = 2048
HEADS = 64
HEAD_DIM = 64
GROUPS = 8
STATE = 128
FF = 5632
CONV = 4
BLOCK_POSITIONS = 128
TOK_DEV = 1024
DI = 4096
TOKENS = 8192
N_TP = 4


def draw_arriving_hidden_sum(key, part):
    noise_key = jax.random.fold_in(key, 11)
    col_key = jax.random.fold_in(key, 12)
    row_key = jax.random.fold_in(key, 13)
    columns = jnp.arange(D, dtype=jnp.float32) / D
    row_scale = jnp.exp(jax.random.uniform(row_key, (TOKENS, 1), jnp.float32, jnp.log(0.4), jnp.log(4.0)))
    base = jnp.clip(jax.random.normal(noise_key, (TOKENS, D), jnp.float32), -6.0, 6.0)
    col_scale = 12.0 ** columns * jnp.exp(jax.random.uniform(col_key, (D,), jnp.float32, -0.35, 0.35))
    return jnp.clip(0.2 * base * row_scale * col_scale, -40.0, 40.0).astype(jnp.bfloat16)


def draw_raw_interval_length(key, part):
    noise_key = jax.random.fold_in(key, 21)
    shift_key = jax.random.fold_in(key, 22)
    shifts = jax.random.uniform(shift_key, (TOKENS // TOK_DEV, 1, 1), jnp.float32, -1.0, 1.0)
    noise = jnp.clip(0.7 * jax.random.normal(noise_key, (TOKENS // TOK_DEV, TOK_DEV, HEADS), jnp.float32), -4.0, 4.0)
    return (noise + shifts).reshape(TOKENS, HEADS).astype(jnp.bfloat16)


def draw_spike_extra_lognoise(key, part):
    spot_key = jax.random.fold_in(key, 31)
    loss_key = jax.random.fold_in(key, 32)
    spots = jax.random.randint(spot_key, (3,), 0, TOKENS)
    losses = jnp.log(jax.random.uniform(loss_key, (3, HEADS), jnp.float32, 0.55, 0.8))
    return jnp.zeros((TOKENS, HEADS), jnp.float32).at[spots].add(losses)


def draw_fading_speed_exponent(key, part):
    pick_key = jax.random.fold_in(key, 41)
    fast_key = jax.random.fold_in(key, 42)
    slow_key = jax.random.fold_in(key, 43)
    share = 0.5
    fast_pick = jax.random.uniform(pick_key, (HEADS,), jnp.float32) < share
    fast_rate = jax.random.uniform(fast_key, (HEADS,), jnp.float32, jnp.log(0.015), jnp.log(0.05))
    slow_rate = jax.random.uniform(slow_key, (HEADS,), jnp.float32, jnp.log(0.15), jnp.log(0.5)) - jnp.log(1.0 * TOKENS)
    return jnp.where(fast_pick, fast_rate, slow_rate)


def steps_of(own_key, shape, cuts, low, largest):
    loudness, own = 1.0, jax.random.fold_in(own_key, 6)
    for dim, parts in cuts:
        heights = jnp.exp(jax.random.uniform(jax.random.fold_in(own, dim), (parts,), jnp.float32, low / len(cuts), largest / len(cuts)))
        loudness = loudness * jnp.repeat(heights, shape[dim] // parts).reshape([-1 if axis == dim else 1 for axis in range(len(shape))])
    return loudness


def centred(key, dims, spread, most, split=(), kind=jnp.bfloat16):
    drawn = spread * jax.random.normal(key, dims, jnp.float32)
    if split:
        drawn = drawn * steps_of(key, dims, split, -0.22, 0.18)
    return jnp.clip(drawn, -most, most).astype(kind)


def setup_inputs(seed: int = 0) -> dict:
    streams_of = jax.random.split(jax.random.key(seed), 18)
    return {
        "arriving_hidden_sum": draw_arriving_hidden_sum(jax.random.fold_in(streams_of[17], 71), 0),
        "content_entries_clustered": centred(streams_of[1], (TOKENS, DI), 1.0, 6.0, ((0, 8), (1, 4))),
        "leaving_switch_entries": centred(streams_of[2], (TOKENS, DI), 1.0, 6.0, ((0, 8), (1, 4))),
        "linked_source_target_pairs": centred(streams_of[3], (TOKENS, GROUPS, 2, STATE), (STATE ** -0.25), 1.78125, ((0, 8), (1, 4))),
        "raw_interval_length": draw_raw_interval_length(jax.random.fold_in(streams_of[17], 71), 0),
        "spike_extra_lognoise": draw_spike_extra_lognoise(jax.random.fold_in(streams_of[17], 71), 0),
        "content_filter_kernel": centred(streams_of[6], (CONV, DI), CONV ** -0.5, 3.0, ((1, 4),)),
        "coupling_filter_kernel": centred(streams_of[7], (CONV, GROUPS, 2, STATE), CONV ** -0.5, 3.0, ((1, 4),)),
        "interval_shift_vector": jnp.clip(jax.random.uniform(streams_of[8], (HEADS,), jnp.float32, -0.5, 0.5) * steps_of(streams_of[8], (HEADS,), ((0, 4),), -0.4, 0.0), -0.5, 0.5),
        "fading_speed_exponent": draw_fading_speed_exponent(jax.random.fold_in(streams_of[17], 71), 0),
        "skip_channel_factor": jnp.clip(jnp.exp(math.log(10.0) - 2.3025851 * jax.random.uniform(streams_of[10], (HEADS,), jnp.float32) ** steps_of(streams_of[10], (HEADS,), ((0, 4),), -0.2, 0.2)), 1.0, 10.0),
        "cluster_rescale_vector": jnp.clip(1.0 + 0.18 * jax.random.normal(streams_of[11], (DI,), jnp.float32), 0.1, 1.9),
        "blender_final_tensor": centred(streams_of[12], (DI, D), DI ** -0.5, 0.09375, ((0, 4),)),
        "prelayer_rescale_vector": jnp.clip(1.0 + 0.18 * jax.random.normal(streams_of[13], (D,), jnp.float32), 0.1, 1.9),
        "switching_linear_tensor": centred(streams_of[14], (D, FF), D ** -0.5, 0.125, ((0, 8), (1, 4))),
        "widening_linear_tensor": centred(streams_of[15], (D, FF), D ** -0.5, 0.125, ((0, 8), (1, 4))),
        "contracting_linear_tensor": centred(streams_of[16], (FF, D), FF ** -0.5, 0.078125, ((0, 4), (1, 8))),
    }


EPS = 1e-06
highest = lax.Precision.HIGHEST

def causal_conv(values, taps):
    taps_count = taps.shape[0]
    length = values.shape[0]
    padded = jnp.pad(values.astype(jnp.float32), ((taps_count - 1, 0), (0, 0)))
    running = jnp.zeros(values.shape, jnp.float32)
    for tap_index in range(taps_count):
        running = running + padded[tap_index:tap_index + length] * taps[tap_index].astype(jnp.float32)
    return jax.nn.silu(running).astype(jnp.bfloat16)

def reference(arriving_hidden_sum, content_entries_clustered, leaving_switch_entries, linked_source_target_pairs, raw_interval_length, spike_extra_lognoise, content_filter_kernel, coupling_filter_kernel, interval_shift_vector, fading_speed_exponent, skip_channel_factor, cluster_rescale_vector, blender_final_tensor, prelayer_rescale_vector, switching_linear_tensor, widening_linear_tensor, contracting_linear_tensor):
    length = content_entries_clustered.shape[0]
    per_group = HEADS // GROUPS
    block_count = length // BLOCK_POSITIONS
    values = causal_conv(content_entries_clustered, content_filter_kernel)
    maps = causal_conv(linked_source_target_pairs.reshape(length, -1), coupling_filter_kernel.reshape(CONV, -1)).reshape(length, GROUPS, 2, STATE)
    write_map = maps[:, :, 0]
    read_map = maps[:, :, 1]
    interval_lengths = jax.nn.softplus(raw_interval_length.astype(jnp.float32) + interval_shift_vector)
    fading_log_factor = -jnp.exp(fading_speed_exponent) * interval_lengths + spike_extra_lognoise
    causal = jnp.tril(jnp.ones((BLOCK_POSITIONS, BLOCK_POSITIONS), bool))

    def block_step(carry_state, inputs):
        value_block, write_block, read_block, step_block, log_block = inputs
        cum_log = jnp.cumsum(log_block, axis=0)
        head_cum = cum_log.T
        log_gap = head_cum[:, :, None] - head_cum[:, None, :]
        intersection = jnp.einsum('lgn,sgn->gls', read_block.astype(jnp.float32), write_block.astype(jnp.float32))
        intersection = jnp.repeat(intersection, per_group, axis=0)
        weights = (intersection * jnp.exp(jnp.where(causal, log_gap, -jnp.inf)) * step_block.T[:, None, :]).astype(jnp.bfloat16)
        within = jnp.einsum('hls,shp->lhp', weights.astype(jnp.float32), value_block.astype(jnp.float32))
        carried = jnp.einsum('lgn,grpn->lgrp', read_block.astype(jnp.float32), carry_state, precision=highest)
        carried = carried.reshape(BLOCK_POSITIONS, HEADS, HEAD_DIM) * jnp.exp(cum_log)[:, :, None]
        end_log = cum_log[-1]
        scaled = (value_block.astype(jnp.float32) * (step_block * jnp.exp(end_log[None, :] - cum_log))[:, :, None]).astype(jnp.bfloat16)
        block_states = jnp.einsum('lgn,lgrp->grpn', write_block.astype(jnp.float32), scaled.astype(jnp.float32).reshape(BLOCK_POSITIONS, GROUPS, per_group, HEAD_DIM))
        carry_state = carry_state * jnp.exp(end_log).reshape(GROUPS, per_group)[:, :, None, None] + block_states
        return (carry_state, within + carried)
    value_heads = values.reshape(length, HEADS, HEAD_DIM)
    inputs = (value_heads.reshape(block_count, BLOCK_POSITIONS, HEADS, HEAD_DIM), write_map.reshape(block_count, BLOCK_POSITIONS, GROUPS, STATE), read_map.reshape(block_count, BLOCK_POSITIONS, GROUPS, STATE), interval_lengths.reshape(block_count, BLOCK_POSITIONS, HEADS), fading_log_factor.reshape(block_count, BLOCK_POSITIONS, HEADS))
    start_state = jnp.zeros((GROUPS, per_group, HEAD_DIM, STATE), jnp.float32)
    _, mixer = lax.scan(block_step, start_state, inputs)
    mixer = mixer.reshape(length, HEADS, HEAD_DIM) + value_heads.astype(jnp.float32) * skip_channel_factor[None, :, None]
    gated = mixer.reshape(length, DI) * jax.nn.silu(leaving_switch_entries.astype(jnp.float32))
    grouped = gated.reshape(length, GROUPS, DI // GROUPS)
    grouped = grouped * lax.rsqrt(lax.optimization_barrier(jnp.mean(grouped * grouped, axis=-1, keepdims=True)) + EPS)
    mixed_rows = (grouped.reshape(length, DI) * cluster_rescale_vector).astype(jnp.bfloat16)
    part_width = DI // N_TP
    mixer_out = jnp.zeros((length, D), jnp.float32)
    for device_rank in range(N_TP):
        partial_sum = jnp.dot(mixed_rows[:, device_rank * part_width:(device_rank + 1) * part_width], blender_final_tensor[device_rank * part_width:(device_rank + 1) * part_width], preferred_element_type=jnp.float32)
        mixer_out = mixer_out + lax.optimization_barrier(partial_sum.astype(jnp.bfloat16)).astype(jnp.float32)
    residual_mid = (arriving_hidden_sum.astype(jnp.float32) + mixer_out).astype(jnp.bfloat16)
    squares = residual_mid.astype(jnp.float32)
    normed = (squares * lax.rsqrt(lax.optimization_barrier(jnp.mean(squares * squares, axis=-1, keepdims=True)) + EPS) * prelayer_rescale_vector).astype(jnp.bfloat16)
    gate_pre = jnp.dot(normed, switching_linear_tensor, preferred_element_type=jnp.float32)
    up_pre = jnp.dot(normed, widening_linear_tensor, preferred_element_type=jnp.float32)
    hidden = (jax.nn.silu(gate_pre) * up_pre).astype(jnp.bfloat16)
    hidden_width = FF // N_TP
    mlp_out = jnp.zeros((length, D), jnp.float32)
    for device_rank in range(N_TP):
        partial_sum = jnp.dot(hidden[:, device_rank * hidden_width:(device_rank + 1) * hidden_width], contracting_linear_tensor[device_rank * hidden_width:(device_rank + 1) * hidden_width], preferred_element_type=jnp.float32)
        mlp_out = mlp_out + lax.optimization_barrier(partial_sum.astype(jnp.bfloat16)).astype(jnp.float32)
    return (residual_mid.astype(jnp.float32) + 0.5 * mlp_out).astype(jnp.bfloat16)
```

```python
import jax
import jax.numpy as jnp
from jax import lax
from jax.experimental import pallas as pl
from jax.experimental.pallas import tpu as pltpu
from jax.sharding import PartitionSpec as P

BLOCK = 128
CORES = 2
EPS = 1e-06
HALO = 16
HIGHEST = lax.Precision.HIGHEST
MESH = pl.DeviceIdType.MESH
VMEM_BYTES = 66_000_000


def ring_shape(count):
    inner = 1
    while inner * inner * 4 <= count:
        inner *= 2
    outer = count // inner
    if inner == 1 or outer % 2:
        return count, 1
    return outer, inner


def ring_at(spot, count):
    outer, inner = ring_shape(count)
    if inner == 1:
        return spot
    if inner == 2:
        late = spot // outer
        return (1 - late) * spot * 2 + late * (2 * (count - 1 - spot) + 1)
    late = jnp.minimum(spot // outer, 1)
    rest = (spot - outer) * late
    lap, step = rest // (inner - 1), rest % (inner - 1)
    odd = lap % 2
    column = (1 + step) * (1 - odd) + (inner - 1 - step) * odd
    return (1 - late) * spot * inner + late * ((outer - 1 - lap) * inner + column)


def ring_spot(index, count):
    outer, inner = ring_shape(count)
    if inner == 1:
        return index
    plane, column = index // inner, index % inner
    late = jnp.minimum(column, 1)
    lap = outer - 1 - plane
    odd = lap % 2
    step = (column - 1) * (1 - odd) + (inner - 1 - column) * odd
    return (1 - late) * plane + late * (outer + lap * (inner - 1) + step)


class Ring:
    def __init__(self, pieces, send_sem, recv_sem):
        count = lax.axis_size("sp")
        me = lax.axis_index("sp")
        spot = ring_spot(me, count)
        self.count, self.hops, self.spot = count, count // 2, spot
        self.pieces, self.send_sem, self.recv_sem = pieces, send_sem, recv_sem
        self.next = (
            ring_at(lax.rem(spot + 1, count), count),
            ring_at(lax.rem(spot + count - 1, count), count),
        )

    def owner(self, way, hop):
        shift = self.count - hop if way == 0 else hop
        return ring_at(lax.rem(self.spot + shift, self.count), self.count)

    def active(self, piece, way, hop):
        return 2 * hop < self.count or piece % 2 == way

    def copy(self, piece, way, hop):
        src, dst = self.pieces[piece](hop == 1, self.owner(way, hop - 1))
        return pltpu.make_async_remote_copy(
            src_ref=src,
            dst_ref=dst,
            send_sem=self.send_sem.at[piece, way, hop - 1],
            recv_sem=self.recv_sem.at[piece, way, hop - 1],
            device_id={"sp": self.next[way]},
            device_id_type=MESH,
        )

    def start(self, piece, hop):
        for way in range(2):
            if self.active(piece, way, hop):
                self.copy(piece, way, hop).start()

    def arrive(self, piece, hop):
        for way in range(2):
            if self.active(piece, way, hop):
                self.copy(piece, way, hop).wait_recv()

    def forward(self, piece, hop):
        self.arrive(piece, hop - 1)
        self.start(piece, hop)

    def drain(self):
        for hop in range(1, self.hops + 1):
            for piece in range(len(self.pieces)):
                for way in range(2):
                    if self.active(piece, way, hop):
                        self.copy(piece, way, hop).wait_send()


def greet(others):
    barrier = pltpu.get_barrier_semaphore()
    for other in others:
        pl.semaphore_signal(barrier, inc=1, device_id=other, device_id_type=MESH)
    pl.semaphore_wait(barrier, len(others))


def peers():
    tp = lax.axis_index("tp")
    chips = lax.axis_size("tp") // CORES
    chip, core = tp // CORES, tp % CORES
    partner = {"tp": chip * CORES + 1 - core}
    across = [{"tp": lax.rem(chip + s, chips) * CORES + core} for s in range(1, chips)]
    return chip, core, partner, across


def silu(x):
    return x / (1.0 + jnp.exp(-x))


def dot(a, b, dims=((1,), (0,)), precision=None):
    return lax.dot_general(
        a, b, (dims, ((), ())), precision=precision, preferred_element_type=jnp.float32
    )


def mixer_kernel(
    arriving, content, leaving, pairs, gate_own, up_own, blend_hbm,
    raw, spike, value_taps, map_taps, shift, fading, skip, rescale,
    mid_out, gate_all, up_all,
    padded, map_padded, leave, blend, arrived, read_maps, mixer, mixed, state, reach, prior,
    messages, partial, from_partner, from_across, mid,
    local_sem, halo_sem, ring_send, ring_recv, state_send, state_recv,
    core_sem, across_sem, mid_sem, out_sem,
):
    length, channels = content.shape
    heads = raw.shape[1]
    size = channels // heads
    groups = read_maps.shape[1] // BLOCK
    wide = channels // groups
    per_group = heads // groups
    taps = value_taps.shape[0]
    blocks = length // BLOCK
    half = length // CORES
    count = lax.axis_size("sp")
    me = lax.axis_index("sp")
    chip, core, partner, across = peers()

    loads = [
        pltpu.make_async_copy(content, padded.at[HALO:], local_sem.at[0]),
        pltpu.make_async_copy(pairs, map_padded.at[HALO:], local_sem.at[1]),
        pltpu.make_async_copy(leaving, leave, local_sem.at[2]),
        pltpu.make_async_copy(blend_hbm, blend, local_sem.at[3]),
        pltpu.make_async_copy(
            arriving.at[pl.ds(pl.multiple_of(core * half, half), half)], arrived, local_sem.at[4]
        ),
    ]
    for load in loads:
        load.start()

    def weight(own, slots):
        return lambda first, owner: (own if first else slots.at[owner], slots.at[owner])

    ring = Ring([weight(gate_own, gate_all), weight(up_own, up_all)], ring_send, ring_recv)
    before = {"sp": lax.rem(me + count - 1, count)}
    after = {"sp": lax.rem(me + 1, count)}
    greet([{"sp": ring.next[0]}, {"sp": ring.next[1]}, before, after, partner, *across])

    def halo(which, src, dst):
        return pltpu.make_async_remote_copy(
            src_ref=src.at[length - HALO :],
            dst_ref=dst.at[:HALO],
            send_sem=halo_sem.at[which, 0],
            recv_sem=halo_sem.at[which, 1],
            device_id=after,
            device_id_type=MESH,
        )

    halos = [halo(0, content, padded), halo(1, pairs, map_padded)]

    @pl.when(me < count - 1)
    def _():
        for h in halos:
            h.start()

    ring.start(0, 1)
    ring.start(1, 1)

    @pl.when(me == 0)
    def _():
        padded[:HALO] = jnp.zeros((HALO, channels), padded.dtype)
        map_padded[:HALO] = jnp.zeros((HALO, map_padded.shape[1]), padded.dtype)

    state[...] = jnp.zeros_like(state)
    prior[...] = jnp.zeros_like(prior)
    loads[0].wait()
    loads[1].wait()

    @pl.when(me > 0)
    def _():
        for h in halos:
            h.wait_recv()

    def expand(per_head):
        head = lax.broadcasted_iota(jnp.int32, (heads, channels), 0)
        place = lax.broadcasted_iota(jnp.int32, (heads, channels), 1) // size
        spread = jnp.where(head == place, 1.0, 0.0)
        return dot(per_head, spread, precision=HIGHEST)

    def conv(ref, taps_ref, start, first, width):
        x = ref[pl.ds(start, BLOCK + HALO), first : first + width].astype(jnp.float32)
        total = x[HALO:] * taps_ref[taps - 1 : taps, first : first + width].astype(jnp.float32)
        for tap in range(taps - 1):
            moved = pltpu.roll(x, taps - 1 - tap, 0)[HALO:]
            total += moved * taps_ref[tap : tap + 1, first : first + width].astype(jnp.float32)
        return silu(total).astype(jnp.bfloat16)

    row = lax.broadcasted_iota(jnp.int32, (BLOCK, BLOCK), 0)
    column = lax.broadcasted_iota(jnp.int32, (BLOCK, BLOCK), 1)
    causal = row >= column
    low = column < size

    def block_step(block, _):
        start = pl.multiple_of(block * BLOCK, BLOCK)
        rows = pl.ds(start, BLOCK)
        raised = raw[rows, :].astype(jnp.float32) + shift[...]
        step = jnp.maximum(raised, 0.0) + jnp.log1p(jnp.exp(-jnp.abs(raised)))
        log_decay = -jnp.exp(fading[...]) * step + spike[rows, :]
        cum = dot(jnp.where(causal, 1.0, 0.0), log_decay, precision=HIGHEST)
        end = cum[BLOCK - 1 : BLOCK, :]
        cum_rows = jnp.transpose(cum)
        step_rows = jnp.transpose(step)
        reach[rows, :] = jnp.exp(cum + prior[0:1, :])
        scale = expand(step * jnp.exp(end - cum))
        grow = expand(jnp.exp(cum))
        small = jnp.concatenate(
            [jnp.exp(end), skip[...], jnp.zeros((6, heads), jnp.float32)], axis=0
        )
        small = expand(small)
        keep, direct = small[0:1], small[1:2]
        prior[...] += end
        for group in range(groups):
            maps = conv(map_padded, map_taps, start, group * 2 * BLOCK, 2 * BLOCK)
            write, read = maps[:, :BLOCK], maps[:, BLOCK:]
            read_maps[rows, group * BLOCK : (group + 1) * BLOCK] = read
            inter = dot(read, write, ((1,), (1,)))
            first = group * wide
            held = state[:, first : first + wide]
            carried = dot(read, held.astype(jnp.bfloat16))
            parts = []
            for pair in range(per_group // 2):
                place = first + pair * 2 * size
                value = conv(padded, value_taps, start, place, 2 * size)
                sides = []
                for side in range(2):
                    h = group * per_group + 2 * pair + side
                    gap = cum[:, h : h + 1] - cum_rows[h : h + 1, :]
                    sides.append(
                        (
                            inter
                            * jnp.exp(jnp.where(causal, gap, -1e30))
                            * step_rows[h : h + 1, :]
                        ).astype(jnp.bfloat16)
                    )
                zero = jnp.zeros_like(value)
                stacked = jnp.concatenate(
                    [jnp.where(low, value, zero), jnp.where(low, zero, value)], axis=0
                )
                within = dot(jnp.concatenate(sides, axis=1), stacked)
                value = value.astype(jnp.float32)
                span = slice(place, place + 2 * size)
                local = slice(pair * 2 * size, (pair + 1) * 2 * size)
                mixer[rows, span] = (
                    within + carried[:, local] * grow[:, span] + direct[:, span] * value
                )
                parts.append((value * scale[:, span]).astype(jnp.bfloat16))
            scaled = jnp.concatenate(parts, axis=1)
            added = dot(write, scaled, ((0,), (0,)))
            state[:, first : first + wide] = held * keep[:, first : first + wide] + added
        return 0

    lax.fori_loop(0, blocks, block_step, 0)

    total = expand(prior[...])[0:1]
    upper = total.astype(jnp.bfloat16)
    rest = total - upper.astype(jnp.float32)
    middle = rest.astype(jnp.bfloat16)
    lower = (rest - middle.astype(jnp.float32)).astype(jnp.bfloat16)
    messages[me, :BLOCK] = state[...].astype(jnp.bfloat16)
    messages[me, BLOCK:] = jnp.concatenate(
        [upper, middle, lower, jnp.zeros((HALO - 3, channels), jnp.bfloat16)], axis=0
    )

    def message(part):
        span = pl.ds(part * (channels // 2), channels // 2)

        def refs(first, owner):
            return messages.at[owner, :, span], messages.at[owner, :, span]

        return refs

    scan = Ring([message(0), message(1)], state_send, state_recv)
    for part in range(2):
        scan.start(part, 1)
    for hop in range(2, scan.hops + 1):
        for part in range(2):
            scan.forward(part, hop)
    for piece in range(2):
        ring.forward(piece, 2)
    for part in range(2):
        scan.arrive(part, scan.hops)

    incoming = jnp.zeros((BLOCK, channels), jnp.float32)
    log = jnp.zeros((1, channels), jnp.float32)
    for device in reversed(range(count - 1)):
        counts = jnp.full((1, channels), device, jnp.int32) < me
        theirs = messages[device, :BLOCK].astype(jnp.float32)
        logs = messages[device, BLOCK:].astype(jnp.float32)
        incoming += jnp.where(counts, theirs * jnp.exp(log), 0.0)
        log += jnp.where(counts, logs[0:1] + logs[1:2] + logs[2:3], 0.0)
    state[...] = incoming

    loads[2].wait()
    loads[3].wait()
    blend_width = blend.shape[1]
    pace = 512 if blend_width % 512 == 0 else blend_width

    def project(side, j):
        turn = (core + 1 + side) % CORES
        start = pl.multiple_of(turn * half + j * BLOCK, BLOCK)
        rows = pl.ds(start, BLOCK)
        grow = expand(reach[rows, :])
        for group in range(groups):
            span = slice(group * wide, (group + 1) * wide)
            read = read_maps[rows, group * BLOCK : (group + 1) * BLOCK]
            more = dot(read, state[:, span].astype(jnp.bfloat16)) * grow[:, span]
            gated = (mixer[rows, span] + more) * silu(leave[rows, span].astype(jnp.float32))
            mean = jnp.mean(gated * gated, axis=1, keepdims=True)
            mixed[:, span] = (gated * lax.rsqrt(mean + EPS) * rescale[:, span]).astype(jnp.bfloat16)
        for first in range(0, blend_width, pace):
            partial[side, j, :, first : first + pace] = dot(
                mixed[...], blend[:, first : first + pace]
            ).astype(jnp.bfloat16)

    def to_partner(j):
        return pltpu.make_async_remote_copy(
            src_ref=partial.at[0, j],
            dst_ref=from_partner.at[j],
            send_sem=core_sem.at[0, j],
            recv_sem=core_sem.at[1, j],
            device_id=partner,
            device_id_type=MESH,
        )

    def to_across(s, j):
        return pltpu.make_async_remote_copy(
            src_ref=partial.at[1, j],
            dst_ref=from_across.at[s, j],
            send_sem=across_sem.at[0, s, j],
            recv_sem=across_sem.at[1, s, j],
            device_id=across[s],
            device_id_type=MESH,
        )

    def mid_rows(j):
        return pl.ds(pl.multiple_of(core * half + j * BLOCK, BLOCK), BLOCK)

    def share_mid(j):
        return pltpu.make_async_remote_copy(
            src_ref=mid.at[mid_rows(j)],
            dst_ref=mid.at[mid_rows(j)],
            send_sem=mid_sem.at[0, j],
            recv_sem=mid_sem.at[1, j],
            device_id=partner,
            device_id_type=MESH,
        )

    half_blocks = half // BLOCK

    def exchange_step(j, _):
        project(0, j)
        to_partner(j).start()
        project(1, j)
        to_partner(j).wait_recv()
        partial[1, j] = (
            partial[1, j].astype(jnp.float32) + from_partner[j].astype(jnp.float32)
        ).astype(jnp.bfloat16)
        for s in range(len(across)):
            to_across(s, j).start()
        return 0

    def collect_step(j, _):
        total = partial[1, j].astype(jnp.float32)
        for s in range(len(across)):
            to_across(s, j).wait_recv()
            total += from_across[s, j].astype(jnp.float32)
        own = arrived[pl.ds(pl.multiple_of(j * BLOCK, BLOCK), BLOCK)].astype(jnp.float32)
        mid[mid_rows(j)] = (own + total).astype(jnp.bfloat16)
        share_mid(j).start()
        return 0

    lax.fori_loop(0, half_blocks // 2, exchange_step, 0)
    if ring.hops >= 3:
        ring.forward(0, 3)
    lax.fori_loop(half_blocks // 2, half_blocks, exchange_step, 0)
    if ring.hops >= 3:
        ring.forward(1, 3)
    loads[4].wait()
    lax.fori_loop(0, half_blocks // 2, collect_step, 0)
    for hop in range(4, ring.hops):
        for piece in range(2):
            ring.forward(piece, hop)
    if ring.hops >= 4:
        ring.forward(0, ring.hops)
    lax.fori_loop(half_blocks // 2, half_blocks, collect_step, 0)
    if ring.hops >= 4:
        ring.forward(1, ring.hops)
    for j in range(half_blocks):
        share_mid(j).wait_recv()
    out = pltpu.make_async_copy(mid, mid_out, out_sem)
    out.start()
    for j in range(half_blocks):
        to_partner(j).wait_send()
        share_mid(j).wait_send()
        for s in range(len(across)):
            to_across(s, j).wait_send()
    scan.drain()

    @pl.when(me < count - 1)
    def _():
        for h in halos:
            h.wait_send()

    for piece in range(2):
        ring.arrive(piece, ring.hops)
    ring.drain()
    out.wait()


def feed_kernel(
    mid_hbm, gain, gate_own, up_own, down_own, gate_all, up_all,
    out,
    mid, normed, gate, up, hidden, down, made, from_partner, from_across,
    local_sem, gate_sem, up_sem, ring_send, ring_recv, core_sem, across_sem,
):
    length, width = mid.shape
    count = lax.axis_size("sp")
    me = lax.axis_index("sp")
    tp = lax.axis_index("tp")
    per_tp = count // lax.axis_size("tp")
    chip, core, partner, across = peers()
    chips = len(across) + 1
    depth = gate_own.shape[0]
    units, cut = down_own.shape
    part_units = units // 2

    first_load = pltpu.make_async_copy(mid_hbm, mid, local_sem.at[0])
    first_load.start()

    def load(device, own, slots, into, sem):
        rows = into.at[device * depth : (device + 1) * depth]

        @pl.when(me == device)
        def _():
            pltpu.make_async_copy(own, rows, sem.at[device]).start()

        @pl.when(me != device)
        def _():
            pltpu.make_async_copy(slots.at[device], rows, sem.at[device]).start()

    for device in range(count):
        load(device, gate_own, gate_all, gate, gate_sem)
        load(device, up_own, up_all, up, up_sem)
    own_down = pltpu.make_async_copy(down_own, down.at[me], local_sem.at[1])
    own_down.start()

    def piece(part):
        rows = pl.ds(part * part_units, part_units)

        def refs(first, owner):
            return (
                down_own.at[rows] if first else down.at[owner, rows],
                down.at[owner, rows],
            )

        return refs

    ring = Ring([piece(0), piece(1)], ring_send, ring_recv)
    greet([{"sp": ring.next[0]}, {"sp": ring.next[1]}, partner, *across])
    for part in range(2):
        ring.start(part, 1)

    first_load.wait()

    def norm_step(block, _):
        rows = pl.ds(pl.multiple_of(block * BLOCK, BLOCK), BLOCK)
        x = mid[rows, :].astype(jnp.float32)
        mean = jnp.mean(x * x, axis=1, keepdims=True)
        normed[rows, :] = (x * lax.rsqrt(mean + EPS) * gain[...]).astype(jnp.bfloat16)
        return 0

    lax.fori_loop(0, length // BLOCK, norm_step, 0)
    for device in range(count):
        rows = slice(device * depth, (device + 1) * depth)
        pltpu.make_async_copy(gate_own, gate.at[rows], gate_sem.at[device]).wait()
        pltpu.make_async_copy(up_own, up.at[rows], up_sem.at[device]).wait()
    own_down.wait()

    tall = 256

    def hidden_step(tile, _):
        rows = pl.ds(pl.multiple_of(tile * tall, tall), tall)
        x = normed[rows, :]
        hidden[rows, :] = (silu(dot(x, gate[...])) * dot(x, up[...])).astype(jnp.bfloat16)
        return 0

    tiles = length // tall
    lax.fori_loop(0, tiles // 4, hidden_step, 0)
    ring.forward(0, 2)
    lax.fori_loop(tiles // 4, 3 * tiles // 4, hidden_step, 0)
    ring.forward(1, 2)
    lax.fori_loop(3 * tiles // 4, tiles, hidden_step, 0)

    order = [(me, 0)]
    for hop in range(1, ring.hops + 1):
        order.append((ring.owner(0, hop), hop))
        if 2 * hop < count:
            order.append((ring.owner(1, hop), hop))

    def target(k):
        goal = order[k][0] // per_tp
        return goal, goal // CORES, goal % CORES

    def over_cores(k):
        return pltpu.make_async_remote_copy(
            src_ref=made.at[k],
            dst_ref=from_partner.at[k],
            send_sem=core_sem.at[0, k],
            recv_sem=core_sem.at[1, k],
            device_id=partner,
            device_id_type=MESH,
        )

    def over_chips(k, s):
        return pltpu.make_async_remote_copy(
            src_ref=made.at[k],
            dst_ref=from_across.at[chips - 2 - s, k],
            send_sem=across_sem.at[0, s, k],
            recv_sem=across_sem.at[1, chips - 2 - s, k],
            device_id=across[s],
            device_id_type=MESH,
        )

    def from_chips(k, s):
        return pltpu.make_async_remote_copy(
            src_ref=made.at[k],
            dst_ref=from_across.at[s, k],
            send_sem=across_sem.at[0, s, k],
            recv_sem=across_sem.at[1, s, k],
            device_id=across[s],
            device_id_type=MESH,
        )

    def make(k):
        def tile_step(tile, _):
            rows = pl.ds(pl.multiple_of(tile * tall, tall), tall)
            made[k, rows, :] = dot(hidden[rows, :], down[order[k][0]]).astype(jnp.bfloat16)
            return 0

        lax.fori_loop(0, tiles, tile_step, 0)

        @pl.when(target(k)[2] != core)
        def _():
            over_cores(k).start()

    def combine(k):
        goal, goal_chip, goal_core = target(k)

        @pl.when(goal_core == core)
        def _():
            over_cores(k).wait_recv()
            made[k] = (
                made[k].astype(jnp.float32) + from_partner[k].astype(jnp.float32)
            ).astype(jnp.bfloat16)
            for s in range(chips - 1):

                @pl.when(goal_chip == lax.rem(chip + s + 1, chips))
                def _():
                    over_chips(k, s).start()

    def finish(k):
        owner = order[k][0]

        @pl.when(target(k)[0] == tp)
        def _():
            total = made[k].astype(jnp.float32)
            for s in range(chips - 1):
                from_chips(k, s).wait_recv()
                total += from_across[s, k].astype(jnp.float32)
            at = pl.ds(pl.multiple_of(owner * cut, cut), cut)
            to = pl.ds(pl.multiple_of(lax.rem(owner, per_tp) * cut, cut), cut)
            out[:, to] = (mid[:, at].astype(jnp.float32) + 0.5 * total).astype(jnp.bfloat16)

    done = 0
    make(0)
    for hop in range(1, ring.hops + 1):
        if hop + 1 <= ring.hops and hop > 1:
            ring.forward(0, hop + 1)
            ring.forward(1, hop + 1)
        elif hop == ring.hops:
            ring.arrive(0, hop)
            ring.arrive(1, hop)
        for k in range(len(order)):
            if order[k][1] == hop:
                make(k)
                combine(k - 1)
                if k >= 3:
                    finish(k - 3)
    last = len(order) - 1
    combine(last)
    for k in range(max(last - 2, 0), last + 1):
        finish(k)
    for k in range(last + 1):
        goal, goal_chip, goal_core = target(k)

        @pl.when(goal_core != core)
        def _():
            over_cores(k).wait_send()

        for s in range(chips - 1):

            @pl.when((goal_core == core) & (goal_chip == lax.rem(chip + s + 1, chips)))
            def _():
                over_chips(k, s).wait_send()

    ring.drain()


def shards(
    arriving, content, leaving, linked, raw, spike, value_taps, map_taps,
    shift, fading, skip, rescale, blend, gain, gate, up, down,
):
    length, channels = content.shape
    heads = raw.shape[1]
    groups, state_size = linked.shape[1], linked.shape[3]
    map_width = groups * 2 * state_size
    width = arriving.shape[1]
    taps = value_taps.shape[0]
    count = lax.axis_size("sp")
    hops = count // 2
    chips = lax.axis_size("tp") // CORES
    half = length // CORES
    half_blocks = half // BLOCK
    depth, units = gate.shape
    cut = down.shape[1]
    anywhere = pl.BlockSpec(memory_space=pl.ANY)
    inside = pl.BlockSpec(memory_space=pltpu.VMEM)
    bf16, f32 = jnp.bfloat16, jnp.float32
    dma = pltpu.SemaphoreType.DMA
    mid, gate_all, up_all = pl.pallas_call(
        mixer_kernel,
        out_shape=(
            jax.ShapeDtypeStruct((length, width), bf16),
            jax.ShapeDtypeStruct((count, depth, units), bf16),
            jax.ShapeDtypeStruct((count, depth, units), bf16),
        ),
        in_specs=[anywhere] * 7 + [inside] * 8,
        out_specs=(anywhere,) * 3,
        scratch_shapes=[
            pltpu.VMEM((HALO + length, channels), bf16),
            pltpu.VMEM((HALO + length, map_width), bf16),
            pltpu.VMEM((length, channels), bf16),
            pltpu.VMEM((channels, width), bf16),
            pltpu.VMEM((half, width), bf16),
            pltpu.VMEM((length, groups * state_size), bf16),
            pltpu.VMEM((length, channels), f32),
            pltpu.VMEM((BLOCK, channels), bf16),
            pltpu.VMEM((state_size, channels), f32),
            pltpu.VMEM((length, heads), f32),
            pltpu.VMEM((8, heads), f32),
            pltpu.VMEM((count, state_size + HALO, channels), bf16),
            pltpu.VMEM((CORES, half_blocks, BLOCK, width), bf16),
            pltpu.VMEM((half_blocks, BLOCK, width), bf16),
            pltpu.VMEM((chips - 1, half_blocks, BLOCK, width), bf16),
            pltpu.VMEM((length, width), bf16),
            dma((5,)),
            dma((2, 2)),
            dma((2, 2, hops)),
            dma((2, 2, hops)),
            dma((2, 2, hops)),
            dma((2, 2, hops)),
            dma((2, half_blocks)),
            dma((2, chips - 1, half_blocks)),
            dma((2, half_blocks)),
            dma(()),
        ],
        compiler_params=pltpu.CompilerParams(
            collective_id=0, has_side_effects=True, vmem_limit_bytes=VMEM_BYTES
        ),
        name="mixer",
    )(
        arriving, content, leaving, linked.reshape(length, map_width), gate, up, blend,
        raw, spike, value_taps, map_taps.reshape(taps, map_width),
        shift[None], fading[None], skip[None], rescale[None],
    )
    return pl.pallas_call(
        feed_kernel,
        out_shape=jax.ShapeDtypeStruct((length, width // lax.axis_size("tp")), bf16),
        in_specs=[anywhere, inside] + [anywhere] * 5,
        out_specs=inside,
        scratch_shapes=[
            pltpu.VMEM((length, width), bf16),
            pltpu.VMEM((length, width), bf16),
            pltpu.VMEM((width, units), bf16),
            pltpu.VMEM((width, units), bf16),
            pltpu.VMEM((length, units), bf16),
            pltpu.VMEM((count, units, cut), bf16),
            pltpu.VMEM((count, length, cut), bf16),
            pltpu.VMEM((count, length, cut), bf16),
            pltpu.VMEM((chips - 1, count, length, cut), bf16),
            dma((2,)),
            dma((count,)),
            dma((count,)),
            dma((2, 2, hops)),
            dma((2, 2, hops)),
            dma((2, count)),
            dma((2, chips - 1, count)),
        ],
        compiler_params=pltpu.CompilerParams(
            collective_id=1, has_side_effects=True, vmem_limit_bytes=VMEM_BYTES
        ),
        name="feed",
    )(mid, gain[None], gate, up, down, gate_all, up_all)


def solution(mesh):
    placed = (
        P("sp", None),
        P("sp", "tp"),
        P("sp", "tp"),
        P("sp", "tp", None, None),
        P("sp", "tp"),
        P("sp", "tp"),
        P(None, "tp"),
        P(None, "tp", None, None),
        P("tp"),
        P("tp"),
        P("tp"),
        P("tp"),
        P("tp", None),
        P(),
        P("sp", "tp"),
        P("sp", "tp"),
        P("tp", "sp"),
    )
    return jax.shard_map(
        shards, mesh=mesh, in_specs=placed, out_specs=P("sp", "tp"), check_vma=False
    )
```

```python
import jax
import jax.numpy as jnp
from jax import lax
from jax.experimental import pallas as pl
from jax.experimental.pallas import tpu as pltpu
from jax.sharding import PartitionSpec as P

BLOCK = 128
CORES = 2
EPS = 1e-06
HALO = 16
HIGHEST = lax.Precision.HIGHEST
MESH = pl.DeviceIdType.MESH
VMEM_BYTES = 64_500_000


def ring_shape(count):
    inner = 1
    while inner * inner * 4 <= count:
        inner *= 2
    outer = count // inner
    if inner == 1 or outer % 2:
        return count, 1
    return outer, inner


def ring_at(spot, count):
    outer, inner = ring_shape(count)
    if inner == 1:
        return spot
    if inner == 2:
        late = spot // outer
        return (1 - late) * spot * 2 + late * (2 * (count - 1 - spot) + 1)
    late = jnp.minimum(spot // outer, 1)
    rest = (spot - outer) * late
    lap, step = rest // (inner - 1), rest % (inner - 1)
    odd = lap % 2
    column = (1 + step) * (1 - odd) + (inner - 1 - step) * odd
    return (1 - late) * spot * inner + late * ((outer - 1 - lap) * inner + column)


def ring_spot(index, count):
    outer, inner = ring_shape(count)
    if inner == 1:
        return index
    plane, column = index // inner, index % inner
    late = jnp.minimum(column, 1)
    lap = outer - 1 - plane
    odd = lap % 2
    step = (column - 1) * (1 - odd) + (inner - 1 - column) * odd
    return (1 - late) * plane + late * (outer + lap * (inner - 1) + step)


PIECES = 4
PARTS = 2
DEPTH = 3


class Flow:
    def __init__(self, sets, send_sem, recv_sem):
        count = lax.axis_size("sp")
        spot = ring_spot(lax.axis_index("sp"), count)
        self.count, self.hops, self.spot = count, count // 2, spot
        self.send_sem, self.recv_sem = send_sem, recv_sem
        self.pieces = [piece for group in sets for piece in group]
        self.next = (
            ring_at(lax.rem(spot + 1, count), count),
            ring_at(lax.rem(spot + count - 1, count), count),
        )
        self.order, self.ends = ([], []), []
        first = 0
        for group in sets:
            for hop in range(1, self.hops + 1):
                for piece in range(first, first + len(group)):
                    for way in range(2):
                        if 2 * hop < count or piece % 2 == way:
                            self.order[way].append((piece, hop))
                self.ends.append(len(self.order[0]))
            first += len(group)
        self.total = len(self.order[0])
        self.pushed = self.pulled = 0

    def owner(self, way, hop):
        shift = self.count - hop if way == 0 else hop
        return ring_at(lax.rem(self.spot + shift, self.count), self.count)

    def copy(self, way, step):
        piece, hop = self.order[way][step]
        src, dst = self.pieces[piece](hop == 1, self.owner(way, hop - 1))
        return pltpu.make_async_remote_copy(
            src_ref=src,
            dst_ref=dst,
            send_sem=self.send_sem.at[piece, way, hop - 1],
            recv_sem=self.recv_sem.at[piece, way, hop - 1],
            device_id={"sp": self.next[way]},
            device_id_type=MESH,
        )

    def push(self):
        if self.pushed < self.total:
            for way in range(2):
                piece, hop = self.order[way][self.pushed]
                while hop > 1 and self.pulled <= self.order[way].index((piece, hop - 1)):
                    self.pull()
            for way in range(2):
                self.copy(way, self.pushed).start()
            self.pushed += 1

    def pull(self):
        if self.pulled < self.total:
            for way in range(2):
                self.copy(way, self.pulled).wait_recv()
            self.pulled += 1

    def step(self, times=1):
        for _ in range(times):
            self.pull()
            self.push()

    def until(self, pulled):
        while self.pulled < pulled:
            self.step()

    def paced(self, index, counts):
        for i, times in enumerate(counts):
            if times:

                @pl.when(index == i)
                def _():
                    self.step(times)

    def drain(self):
        for step in range(self.total):
            for way in range(2):
                self.copy(way, step).wait_send()


def greet(others):
    barrier = pltpu.get_barrier_semaphore()
    for other in others:
        pl.semaphore_signal(barrier, inc=1, device_id=other, device_id_type=MESH)
    pl.semaphore_wait(barrier, len(others))


def peers():
    tp = lax.axis_index("tp")
    chips = lax.axis_size("tp") // CORES
    chip, core = tp // CORES, tp % CORES
    partner = {"tp": chip * CORES + 1 - core}
    across = [{"tp": lax.rem(chip + s, chips) * CORES + core} for s in range(1, chips)]
    return chip, core, partner, across


def silu(x):
    return x / (1.0 + jnp.exp(-x))


def dot(a, b, dims=((1,), (0,)), precision=None):
    return lax.dot_general(
        a, b, (dims, ((), ())), precision=precision, preferred_element_type=jnp.float32
    )


def layer_kernel(
    arriving, content, leaving, pairs, gate_own, up_own, down_own, blend_hbm,
    raw, spike, value_taps, map_taps, shift, fading, skip, rescale, gain,
    out,
    padded, map_padded, regroup, leave, blend, arrived, read_maps, mixer, mixed, state, reach, prior,
    messages, chain, partial, from_partner, from_across, mid, resid,
    gate, up, hidden, down, made, made_partner, made_across,
    local_sem, halo_sem, ring_send, ring_recv, plane_send, plane_recv, chain_sem,
    core_sem, across_sem, mid_sem, made_core_sem, made_across_sem,
):
    length, channels = content.shape
    heads = raw.shape[0]
    size = channels // heads
    groups = read_maps.shape[1] // BLOCK
    wide = channels // groups
    per_group = heads // groups
    taps = value_taps.shape[0]
    kinds = groups * 2
    blocks = length // BLOCK
    half = length // CORES
    half_blocks = half // BLOCK
    count = lax.axis_size("sp")
    me = lax.axis_index("sp")
    tp = lax.axis_index("tp")
    per_tp = count // lax.axis_size("tp")
    chip, core, partner, across = peers()
    chips = len(across) + 1
    depth = gate_own.shape[0]
    planes, inner = ring_shape(count)
    plane, spoke = me // inner, lax.rem(me, inner)
    sides, units = down.shape[1], down.shape[2]

    loads = [
        pltpu.make_async_copy(content, padded.at[HALO:], local_sem.at[0]),
        pltpu.make_async_copy(pairs, map_padded.at[HALO * kinds :], local_sem.at[1]),
        pltpu.make_async_copy(leaving, leave, local_sem.at[2]),
        pltpu.make_async_copy(blend_hbm, blend, local_sem.at[3]),
        pltpu.make_async_copy(
            arriving.at[pl.ds(pl.multiple_of(core * half, half), half)], arrived, local_sem.at[4]
        ),
    ]
    mine = pl.ds(pl.multiple_of(me * depth, depth), depth)
    loads.append(pltpu.make_async_copy(gate_own, gate.at[mine], local_sem.at[5]))
    loads.append(pltpu.make_async_copy(up_own, up.at[mine], local_sem.at[6]))
    for side in range(sides):
        loads.append(
            pltpu.make_async_copy(
                down_own.at[:, pl.ds(side * BLOCK, BLOCK)], down.at[me, side], local_sem.at[7 + side]
            )
        )
    loads[0].start()
    loads[1].start()

    def rows_piece(own, whole, part):
        tall = depth // PIECES

        def refs(first, owner):
            at = pl.multiple_of(owner * depth + part * tall, tall)
            target = whole.at[pl.ds(at, tall)]
            return (own.at[pl.ds(part * tall, tall)] if first else target), target

        return refs

    def down_piece(side, part):
        rows = pl.ds(part * (units // 2), units // 2)

        def refs(first, owner):
            target = down.at[owner, side, rows]
            source = down_own.at[rows, pl.ds(side * BLOCK, BLOCK)]
            return (source if first else target), target

        return refs

    flow = Flow(
        [
            [rows_piece(gate_own, gate, part) for part in range(PIECES)]
            + [rows_piece(up_own, up, part) for part in range(PIECES)],
            [down_piece(side, part) for side in range(sides) for part in range(2)],
        ],
        ring_send,
        ring_recv,
    )
    fed = flow.ends[flow.hops - 1]
    before = {"sp": lax.rem(me + count - 1, count)}
    after = {"sp": lax.rem(me + 1, count)}
    siblings = [{"sp": plane * inner + lax.rem(spoke + s, inner)} for s in range(1, inner)]
    below = {"sp": lax.rem(me + inner, count)}
    above = {"sp": lax.rem(me + count - inner, count)}
    greet(
        [
            {"sp": flow.next[0]}, {"sp": flow.next[1]}, before, after, below, above,
            partner, *across, *siblings,
        ]
    )

    def halo(which, src, dst, rows):
        return pltpu.make_async_remote_copy(
            src_ref=src.at[src.shape[0] - rows :],
            dst_ref=dst.at[:rows],
            send_sem=halo_sem.at[which, 0],
            recv_sem=halo_sem.at[which, 1],
            device_id=after,
            device_id_type=MESH,
        )

    halos = [halo(0, content, padded, HALO), halo(1, pairs, map_padded, HALO * kinds)]

    @pl.when(me < count - 1)
    def _():
        for h in halos:
            h.start()

    for _ in range(DEPTH):
        flow.push()
    for load in loads[2:]:
        load.start()

    @pl.when(me == 0)
    def _():
        padded[:HALO] = jnp.zeros((HALO, channels), padded.dtype)
        map_padded[: HALO * kinds] = jnp.zeros((HALO * kinds, BLOCK), padded.dtype)

    to = lax.broadcasted_iota(jnp.int32, regroup.shape, 0)
    at = lax.broadcasted_iota(jnp.int32, regroup.shape, 1)
    regroup[...] = jnp.where(to == lax.rem(at, kinds) * BLOCK + at // kinds, 1.0, 0.0).astype(
        jnp.bfloat16
    )
    state[...] = jnp.zeros_like(state)
    prior[...] = jnp.zeros_like(prior)
    loads[0].wait()
    loads[1].wait()

    @pl.when(me > 0)
    def _():
        for h in halos:
            h.wait_recv()

    head = lax.broadcasted_iota(jnp.int32, (heads, channels), 0)
    place = lax.broadcasted_iota(jnp.int32, (heads, channels), 1) // size
    spread = jnp.where(head == place, 1.0, 0.0).astype(jnp.bfloat16)
    spread = jnp.concatenate([spread] * 3, axis=0)

    def expand(per_head):
        upper = per_head.astype(jnp.bfloat16)
        rest = per_head - upper.astype(jnp.float32)
        middle = rest.astype(jnp.bfloat16)
        lower = (rest - middle.astype(jnp.float32)).astype(jnp.bfloat16)
        return dot(jnp.concatenate([upper, middle, lower], axis=1), spread)

    def conv(ref, weights, start, first, width):
        x = ref[pl.ds(start, BLOCK + HALO), first : first + width].astype(jnp.float32)
        total = x[HALO:] * weights[taps - 1]
        for tap in range(taps - 1):
            total += pltpu.roll(x, taps - 1 - tap, 0)[HALO:] * weights[tap]
        return silu(total).astype(jnp.bfloat16)

    def map_conv(start):
        tall = BLOCK * kinds
        first = pl.multiple_of(start * kinds, tall)
        x = map_padded[pl.ds(first, tall + HALO * kinds), :].astype(jnp.float32)
        total = jnp.zeros((tall // 8, 8, BLOCK), jnp.float32)
        for tap in range(taps):
            line = [
                map_taps[tap, kind // 2, kind % 2 : kind % 2 + 1, :].astype(jnp.float32)
                for kind in range(kinds)
            ]
            weights = jnp.concatenate(line * (8 // kinds), axis=0)
            moved = x if tap == taps - 1 else pltpu.roll(x, (taps - 1 - tap) * kinds, 0)
            total += moved[HALO * kinds :].reshape(total.shape) * weights[None]
        maps = silu(total).reshape(tall, BLOCK).astype(jnp.bfloat16)
        return dot(regroup[...], maps).astype(jnp.bfloat16)

    row = lax.broadcasted_iota(jnp.int32, (BLOCK, BLOCK), 0)
    column = lax.broadcasted_iota(jnp.int32, (BLOCK, BLOCK), 1)
    causal = row >= column
    low = column < size
    running = jnp.where(row <= column, 1.0, 0.0)
    shift_rows = jnp.transpose(jnp.broadcast_to(shift[...], (BLOCK, heads)))
    rate_rows = jnp.transpose(jnp.broadcast_to(-jnp.exp(fading[...]), (BLOCK, heads)))
    direct = expand(jnp.broadcast_to(skip[...], (8, heads)))[0:1]

    def block_step(block, _):
        start = pl.multiple_of(block * BLOCK, BLOCK)
        rows = pl.ds(start, BLOCK)
        raised = raw[:, rows].astype(jnp.float32) + shift_rows
        step_rows = jnp.maximum(raised, 0.0) + jnp.log1p(jnp.exp(-jnp.abs(raised)))
        log_decay = rate_rows * step_rows + spike[:, rows]
        cum_rows = dot(log_decay, running, precision=HIGHEST)
        end = cum_rows[:, BLOCK - 1 : BLOCK]
        reach[:, rows] = jnp.exp(cum_rows + prior[...])
        prior[...] += jnp.broadcast_to(end, prior.shape)
        columns = jnp.transpose(
            jnp.concatenate(
                [cum_rows, step_rows * jnp.exp(end - cum_rows), jnp.exp(cum_rows)], axis=0
            )
        )
        cum = columns[:, :heads]
        scale = expand(columns[:, heads : 2 * heads])
        grow = expand(columns[:, 2 * heads :])
        keep = grow[BLOCK - 1 : BLOCK]
        maps = map_conv(start)
        for group in range(groups):
            write = maps[2 * group * BLOCK : (2 * group + 1) * BLOCK]
            read = maps[(2 * group + 1) * BLOCK : (2 * group + 2) * BLOCK]
            read_maps[rows, group * BLOCK : (group + 1) * BLOCK] = read
            inter = dot(read, write, ((1,), (1,)))
            first = group * wide
            held = state[:, first : first + wide]
            carried = dot(read, held.astype(jnp.bfloat16))
            parts = []
            for pair in range(per_group // 2):
                place = first + pair * 2 * size
                span = slice(place, place + 2 * size)
                weights = [
                    value_taps[tap : tap + 1, span].astype(jnp.float32) for tap in range(taps)
                ]
                value = conv(padded, weights, start, place, 2 * size)
                sides = []
                for side in range(2):
                    h = group * per_group + 2 * pair + side
                    gap = cum[:, h : h + 1] - cum_rows[h : h + 1, :]
                    sides.append(
                        (
                            inter
                            * jnp.exp(jnp.where(causal, gap, -1e30))
                            * step_rows[h : h + 1, :]
                        ).astype(jnp.bfloat16)
                    )
                zero = jnp.zeros_like(value)
                stacked = jnp.concatenate(
                    [jnp.where(low, value, zero), jnp.where(low, zero, value)], axis=0
                )
                within = dot(jnp.concatenate(sides, axis=1), stacked)
                value = value.astype(jnp.float32)
                local = slice(pair * 2 * size, (pair + 1) * 2 * size)
                mixer[rows, span] = (
                    within + carried[:, local] * grow[:, span] + direct[:, span] * value
                )
                parts.append((value * scale[:, span]).astype(jnp.bfloat16))
            scaled = jnp.concatenate(parts, axis=1)
            added = dot(write, scaled, ((0,), (0,)))
            state[:, first : first + wide] = held * keep[:, first : first + wide] + added
        return 0

    def local_step(turn, _):
        lax.fori_loop(2 * turn, 2 * turn + 2, block_step, 0)
        flow.paced(turn, [0, 1, 1, 1])
        return 0

    lax.fori_loop(0, blocks // 2, local_step, 0)

    total = expand(jnp.transpose(prior[...]))[0:1]
    upper = total.astype(jnp.bfloat16)
    rest = total - upper.astype(jnp.float32)
    middle = rest.astype(jnp.bfloat16)
    lower = (rest - middle.astype(jnp.float32)).astype(jnp.bfloat16)
    messages[spoke, BLOCK:] = jnp.concatenate(
        [upper, middle, lower, jnp.zeros((HALO - 3, channels), jnp.bfloat16)], axis=0
    )
    messages[spoke, :BLOCK] = state[...].astype(jnp.bfloat16)

    def to_sibling(s):
        return pltpu.make_async_remote_copy(
            src_ref=messages.at[spoke],
            dst_ref=messages.at[spoke],
            send_sem=plane_send.at[s],
            recv_sem=plane_recv.at[inner - 2 - s],
            device_id=siblings[s],
            device_id_type=MESH,
        )

    for s in range(inner - 1):
        to_sibling(s).start()
    flow.pull()
    flow.step(2)
    for s in range(inner - 1):
        to_sibling(inner - 2 - s).wait_recv()

    bands = 2
    band = channels // bands

    def pass_on(part):
        span = pl.ds(part * band, band)
        return pltpu.make_async_remote_copy(
            src_ref=chain.at[1, :, span],
            dst_ref=chain.at[0, :, span],
            send_sem=chain_sem.at[0, part],
            recv_sem=chain_sem.at[1, part],
            device_id=below,
            device_id_type=MESH,
        )

    def logs_of(other):
        terms = messages[other, BLOCK:].astype(jnp.float32)
        return terms[0:1] + terms[1:2] + terms[2:3]

    logs = [logs_of(other) for other in range(inner)]

    def plane_sum(part, behind):
        span = slice(part * band, (part + 1) * band)
        summed = jnp.zeros((BLOCK, band), jnp.float32)
        log = jnp.zeros((1, band), jnp.float32)
        for other in reversed(range(inner)):
            theirs = messages[other, :BLOCK, span].astype(jnp.float32) * jnp.exp(log)
            if behind:
                counts = jnp.full((1, band), other, jnp.int32) < spoke
                summed += jnp.where(counts, theirs, 0.0)
                log += jnp.where(counts, logs[other][:, span], 0.0)
            else:
                summed += theirs
                log += logs[other][:, span]
        return summed, jnp.exp(log)

    @pl.when(plane == 0)
    def _():
        chain[0] = jnp.zeros((BLOCK, channels), jnp.bfloat16)
        for part in range(bands):
            chain[1, :, part * band : (part + 1) * band] = plane_sum(part, False)[0].astype(
                jnp.bfloat16
            )
            pass_on(part).start()

    for link in range(planes - 1):
        flow.step(3)

        @pl.when(plane == link + 1)
        def _():
            for part in range(bands):
                span = slice(part * band, (part + 1) * band)
                pass_on(part).wait_recv()
                if link + 2 < planes:
                    summed, decay = plane_sum(part, False)
                    chain[1, :, span] = (
                        chain[0, :, span].astype(jnp.float32) * decay + summed
                    ).astype(jnp.bfloat16)
                    pass_on(part).start()

    for part in range(bands):
        span = slice(part * band, (part + 1) * band)
        summed, decay = plane_sum(part, True)
        state[:, span] = chain[0, :, span].astype(jnp.float32) * decay + summed
    flow.push()

    loads[2].wait()
    loads[3].wait()
    blend_width = blend.shape[1]
    pace = 512 if blend_width % 512 == 0 else blend_width

    def project(side, j):
        turn = (core + 1 + side) % CORES
        start = pl.multiple_of(turn * half + j * BLOCK, BLOCK)
        rows = pl.ds(start, BLOCK)
        grow = expand(jnp.transpose(reach[:, rows]))
        for group in range(groups):
            span = slice(group * wide, (group + 1) * wide)
            read = read_maps[rows, group * BLOCK : (group + 1) * BLOCK]
            more = dot(read, state[:, span].astype(jnp.bfloat16)) * grow[:, span]
            gated = (mixer[rows, span] + more) * silu(leave[rows, span].astype(jnp.float32))
            mean = jnp.mean(gated * gated, axis=1, keepdims=True)
            mixed[:, span] = (gated * lax.rsqrt(mean + EPS) * rescale[:, span]).astype(jnp.bfloat16)
        for first in range(0, blend_width, pace):
            partial[side, j, :, first : first + pace] = dot(
                mixed[...], blend[:, first : first + pace]
            ).astype(jnp.bfloat16)

    def to_partner(j):
        return pltpu.make_async_remote_copy(
            src_ref=partial.at[0, j],
            dst_ref=from_partner.at[j],
            send_sem=core_sem.at[0, j],
            recv_sem=core_sem.at[1, j],
            device_id=partner,
            device_id_type=MESH,
        )

    def to_across(s, j):
        return pltpu.make_async_remote_copy(
            src_ref=partial.at[1, j],
            dst_ref=from_across.at[s, j],
            send_sem=across_sem.at[0, s, j],
            recv_sem=across_sem.at[1, s, j],
            device_id=across[s],
            device_id_type=MESH,
        )

    def mid_rows(j):
        return pl.ds(pl.multiple_of(core * half + j * BLOCK, BLOCK), BLOCK)

    def share_mid(j):
        return pltpu.make_async_remote_copy(
            src_ref=mid.at[mid_rows(j)],
            dst_ref=mid.at[mid_rows(j)],
            send_sem=mid_sem.at[0, j],
            recv_sem=mid_sem.at[1, j],
            device_id=partner,
            device_id_type=MESH,
        )

    def exchange_step(j, _):
        project(0, j)
        to_partner(j).start()
        flow.paced(j, [0, 1, 1, 1])
        project(1, j)
        to_partner(j).wait_recv()
        partial[1, j] = (
            partial[1, j].astype(jnp.float32) + from_partner[j].astype(jnp.float32)
        ).astype(jnp.bfloat16)
        for s in range(len(across)):
            to_across(s, j).start()
        return 0

    def collect_step(j, _):
        flow.paced(j, [1, 3, 3, 3])
        total = partial[1, j].astype(jnp.float32)
        for s in range(len(across)):
            to_across(s, j).wait_recv()
            total += from_across[s, j].astype(jnp.float32)
        own = arrived[pl.ds(pl.multiple_of(j * BLOCK, BLOCK), BLOCK)].astype(jnp.float32)
        mid[mid_rows(j)] = (own + total).astype(jnp.bfloat16)
        share_mid(j).start()
        return 0

    lax.fori_loop(0, half_blocks, exchange_step, 0)
    loads[4].wait()
    lax.fori_loop(0, half_blocks, collect_step, 0)
    for j in range(half_blocks):
        share_mid(j).wait_recv()
        share_mid(j).wait_send()
    own_width = resid.shape[1]

    def norm_step(block, _):
        rows = pl.ds(pl.multiple_of(block * BLOCK, BLOCK), BLOCK)
        resid[rows, :] = mid[rows, pl.ds(pl.multiple_of(tp * own_width, own_width), own_width)]
        x = mid[rows, :].astype(jnp.float32)
        mean = jnp.mean(x * x, axis=1, keepdims=True)
        mid[rows, :] = (x * lax.rsqrt(mean + EPS) * gain[...]).astype(jnp.bfloat16)
        return 0

    lax.fori_loop(0, blocks, norm_step, 0)
    for load in loads[5:]:
        load.wait()
    flow.until(fed)

    tall = 256
    tiles = length // tall

    def hidden_step(tile, _):
        rows = pl.ds(pl.multiple_of(tile * tall, tall), tall)
        x = mid[rows, :]
        hidden[rows, :] = (silu(dot(x, gate[...])) * dot(x, up[...])).astype(jnp.bfloat16)
        flow.paced(tile, [1, 1, 1, 1])
        return 0

    lax.fori_loop(0, tiles, hidden_step, 0)

    order = [(me, 0)]
    for hop in range(1, flow.hops + 1):
        order.append((flow.owner(0, hop), hop))
        if 2 * hop < count:
            order.append((flow.owner(1, hop), hop))

    def target(k):
        goal = order[k][0] // per_tp
        return goal // CORES, goal % CORES

    def slot(k):
        owner = order[k][0]
        return owner // (per_tp * CORES) * per_tp + lax.rem(owner, per_tp)

    long = length // PARTS
    units_of = [(side, part) for side in range(sides) for part in range(PARTS)]

    def over_cores(k, unit):
        return pltpu.make_async_remote_copy(
            src_ref=made.at[k, unit],
            dst_ref=made_partner.at[slot(k), unit],
            send_sem=made_core_sem.at[0, k, unit],
            recv_sem=made_core_sem.at[1, k, unit],
            device_id=partner,
            device_id_type=MESH,
        )

    def over_chips(k, unit, s, into):
        return pltpu.make_async_remote_copy(
            src_ref=made.at[k, unit],
            dst_ref=made_across.at[into, lax.rem(order[k][0], per_tp), unit],
            send_sem=made_across_sem.at[0, s, k, unit],
            recv_sem=made_across_sem.at[1, into, k, unit],
            device_id=across[s],
            device_id_type=MESH,
        )

    def make(k, unit):
        side, part = units_of[unit]
        for first in range(0, long, tall):
            rows = slice(part * long + first, part * long + first + tall)
            made[k, unit, first : first + tall, :] = dot(
                hidden[rows, :], down[order[k][0], side]
            ).astype(jnp.bfloat16)

        @pl.when(target(k)[1] != core)
        def _():
            over_cores(k, unit).start()

    def combine(k, unit):
        goal_chip, goal_core = target(k)

        @pl.when(goal_core == core)
        def _():
            over_cores(k, unit).wait_recv()
            made[k, unit] = (
                made[k, unit].astype(jnp.float32) + made_partner[slot(k), unit].astype(jnp.float32)
            ).astype(jnp.bfloat16)
            for s in range(chips - 1):

                @pl.when(goal_chip == lax.rem(chip + s + 1, chips))
                def _():
                    over_chips(k, unit, s, chips - 2 - s).start()

    def finish(k, unit):
        owner = order[k][0]
        side, part = units_of[unit]

        @pl.when(owner // per_tp == tp)
        def _():
            total = made[k, unit].astype(jnp.float32)
            for s in range(chips - 1):
                over_chips(k, unit, s, s).wait_recv()
                total += made_across[s, lax.rem(owner, per_tp), unit].astype(jnp.float32)
            at = (lax.rem(owner, per_tp) * sides + side) * BLOCK
            to = pl.ds(pl.multiple_of(at, BLOCK), BLOCK)
            rows = slice(part * long, (part + 1) * long)
            out[rows, to] = (resid[rows, to].astype(jnp.float32) + 0.5 * total).astype(jnp.bfloat16)

    made_units, summed_units, finished = [], 0, 0

    def sum_up_to(n):
        nonlocal summed_units
        while summed_units < n:
            combine(*made_units[summed_units])
            summed_units += 1

    def finish_up_to(n):
        nonlocal finished
        while finished < n:
            finish(*made_units[finished])
            finished += 1

    def handle(ks, side, lag):
        for k in ks:
            for part in range(PARTS):
                make(k, side * PARTS + part)
                made_units.append((k, side * PARTS + part))
                sum_up_to(len(made_units) - lag)

    lag = 3
    for side in range(sides):
        handle([0], side, lag)
    flow.step()
    for hop in range(1, flow.hops + 1):
        ks = [k for k in range(len(order)) if order[k][1] == hop]
        begin, end = flow.ends[flow.hops + hop - 2], flow.ends[flow.hops + hop - 1]
        old = len(made_units)
        for side in range(sides):
            flow.until(begin + (end - begin) * (side + 1) // sides)
            handle(ks, side, lag)
            if 2 * hop < flow.hops:
                flow.step()
            if hop > 1:
                sum_up_to(len(made_units))
        if hop < flow.hops:
            finish_up_to(old)
    finish_up_to(len(made_units))

    @pl.when(me < count - 1)
    def _():
        for h in halos:
            h.wait_send()

    for s in range(inner - 1):
        to_sibling(s).wait_send()

    @pl.when(plane < planes - 1)
    def _():
        for part in range(bands):
            pass_on(part).wait_send()

    for j in range(half_blocks):
        to_partner(j).wait_send()
        for s in range(len(across)):
            to_across(s, j).wait_send()
    flow.drain()
    for k in range(len(order)):
        goal_chip, goal_core = target(k)

        @pl.when(goal_core != core)
        def _():
            for unit in range(len(units_of)):
                over_cores(k, unit).wait_send()

        for s in range(chips - 1):

            @pl.when((goal_core == core) & (goal_chip == lax.rem(chip + s + 1, chips)))
            def _():
                for unit in range(len(units_of)):
                    over_chips(k, unit, s, chips - 2 - s).wait_send()


def shards(
    arriving, content, leaving, linked, raw, spike, value_taps, map_taps,
    shift, fading, skip, rescale, blend, gain, gate, up, down,
):
    length, channels = content.shape
    heads = raw.shape[1]
    groups, state_size = linked.shape[1], linked.shape[3]
    kinds = groups * 2
    width = arriving.shape[1]
    count = lax.axis_size("sp")
    hops = count // 2
    inner = ring_shape(count)[1]
    tp_count = lax.axis_size("tp")
    chips = tp_count // CORES
    half = length // CORES
    half_blocks = half // BLOCK
    units, cut = down.shape
    sides = cut // BLOCK
    per_tp = count // tp_count
    subs = sides * PARTS
    pieces = 2 * PIECES + 2 * sides
    anywhere = pl.BlockSpec(memory_space=pl.ANY)
    inside = pl.BlockSpec(memory_space=pltpu.VMEM)
    bf16, f32 = jnp.bfloat16, jnp.float32
    dma = pltpu.SemaphoreType.DMA
    return pl.pallas_call(
        layer_kernel,
        out_shape=pltpu.VMEM((length, width // tp_count), bf16),
        in_specs=[anywhere] * 8 + [inside] * 9,
        out_specs=inside,
        scratch_shapes=[
            pltpu.VMEM((HALO + length, channels), bf16),
            pltpu.VMEM(((HALO + length) * kinds, state_size), bf16),
            pltpu.VMEM((BLOCK * kinds, BLOCK * kinds), bf16),
            pltpu.VMEM((length, channels), bf16),
            pltpu.VMEM((channels, width), bf16),
            pltpu.VMEM((half, width), bf16),
            pltpu.VMEM((length, groups * state_size), bf16),
            pltpu.VMEM((length, channels), f32),
            pltpu.VMEM((BLOCK, channels), bf16),
            pltpu.VMEM((state_size, channels), f32),
            pltpu.VMEM((heads, length), f32),
            pltpu.VMEM((heads, BLOCK), f32),
            pltpu.VMEM((inner, state_size + HALO, channels), bf16),
            pltpu.VMEM((2, state_size, channels), bf16),
            pltpu.VMEM((CORES, half_blocks, BLOCK, width), bf16),
            pltpu.VMEM((half_blocks, BLOCK, width), bf16),
            pltpu.VMEM((chips - 1, half_blocks, BLOCK, width), bf16),
            pltpu.VMEM((length, width), bf16),
            pltpu.VMEM((length, width // tp_count), bf16),
            pltpu.VMEM((width, units), bf16),
            pltpu.VMEM((width, units), bf16),
            pltpu.VMEM((length, units), bf16),
            pltpu.VMEM((count, sides, units, BLOCK), bf16),
            pltpu.VMEM((count, subs, length // PARTS, BLOCK), bf16),
            pltpu.VMEM((chips * per_tp, subs, length // PARTS, BLOCK), bf16),
            pltpu.VMEM((chips - 1, per_tp, subs, length // PARTS, BLOCK), bf16),
            dma((7 + sides,)),
            dma((2, 2)),
            dma((pieces, 2, hops)),
            dma((pieces, 2, hops)),
            dma((max(inner - 1, 1),)),
            dma((max(inner - 1, 1),)),
            dma((2, 2)),
            dma((2, half_blocks)),
            dma((2, chips - 1, half_blocks)),
            dma((2, half_blocks)),
            dma((2, count, subs)),
            dma((2, chips - 1, count, subs)),
        ],
        compiler_params=pltpu.CompilerParams(
            collective_id=0, has_side_effects=True, vmem_limit_bytes=VMEM_BYTES
        ),
        name="layer",
    )(
        arriving, content, leaving, linked.reshape(length * kinds, state_size), gate, up, down, blend,
        raw.T, spike.T, value_taps, map_taps,
        shift[None], fading[None], skip[None], rescale[None], gain[None],
    )


def solution(mesh):
    placed = (
        P("sp", None),
        P("sp", "tp"),
        P("sp", "tp"),
        P("sp", "tp", None, None),
        P("sp", "tp"),
        P("sp", "tp"),
        P(None, "tp"),
        P(None, "tp", None, None),
        P("tp"),
        P("tp"),
        P("tp"),
        P("tp"),
        P("tp", None),
        P(),
        P("sp", "tp"),
        P("sp", "tp"),
        P("tp", "sp"),
    )
    return jax.shard_map(
        shards, mesh=mesh, in_specs=placed, out_specs=P("sp", "tp"), check_vma=False
    )
```

```python
import jax
import jax.numpy as jnp
from jax import lax
from jax.experimental import pallas as pl
from jax.experimental.pallas import tpu as pltpu
from jax.sharding import PartitionSpec as P

BLOCK = 128
CORES = 2
EPS = 1e-06
HALO = 16
HIGHEST = lax.Precision.HIGHEST
MESH = pl.DeviceIdType.MESH
VMEM_BYTES = 65_500_000


def ring_shape(count):
    inner = 1
    while inner * inner * 4 <= count:
        inner *= 2
    outer = count // inner
    if inner == 1 or outer % 2:
        return count, 1
    return outer, inner


def ring_at(spot, count):
    outer, inner = ring_shape(count)
    if inner == 1:
        return spot
    if inner == 2:
        late = spot // outer
        return (1 - late) * spot * 2 + late * (2 * (count - 1 - spot) + 1)
    late = jnp.minimum(spot // outer, 1)
    rest = (spot - outer) * late
    lap, step = rest // (inner - 1), rest % (inner - 1)
    odd = lap % 2
    column = (1 + step) * (1 - odd) + (inner - 1 - step) * odd
    return (1 - late) * spot * inner + late * ((outer - 1 - lap) * inner + column)


def ring_spot(index, count):
    outer, inner = ring_shape(count)
    if inner == 1:
        return index
    plane, column = index // inner, index % inner
    late = jnp.minimum(column, 1)
    lap = outer - 1 - plane
    odd = lap % 2
    step = (column - 1) * (1 - odd) + (inner - 1 - column) * odd
    return (1 - late) * plane + late * (outer + lap * (inner - 1) + step)


PIECES = 4
PARTS = 2
SLOTS = 8
DEPTH = 3


class Flow:
    def __init__(self, sets, send_sem, recv_sem):
        count = lax.axis_size("sp")
        spot = ring_spot(lax.axis_index("sp"), count)
        self.count, self.hops, self.spot = count, count // 2, spot
        self.send_sem, self.recv_sem = send_sem, recv_sem
        self.pieces = [piece for group in sets for piece in group]
        self.next = (
            ring_at(lax.rem(spot + 1, count), count),
            ring_at(lax.rem(spot + count - 1, count), count),
        )
        self.order, self.ends = ([], []), []
        first = 0
        for group in sets:
            for hop in range(1, self.hops + 1):
                for piece in range(first, first + len(group)):
                    for way in range(2):
                        if 2 * hop < count or piece % 2 == way:
                            self.order[way].append((piece, hop))
                self.ends.append(len(self.order[0]))
            first += len(group)
        self.total = len(self.order[0])
        self.pushed = self.pulled = 0

    def owner(self, way, hop):
        shift = self.count - hop if way == 0 else hop
        return ring_at(lax.rem(self.spot + shift, self.count), self.count)

    def copy(self, way, step):
        piece, hop = self.order[way][step]
        src, dst = self.pieces[piece](hop == 1, self.owner(way, hop - 1))
        return pltpu.make_async_remote_copy(
            src_ref=src,
            dst_ref=dst,
            send_sem=self.send_sem.at[way, step % SLOTS],
            recv_sem=self.recv_sem.at[way, step % SLOTS],
            device_id={"sp": self.next[way]},
            device_id_type=MESH,
        )

    def push(self):
        if self.pushed < self.total:
            for way in range(2):
                piece, hop = self.order[way][self.pushed]
                while hop > 1 and self.pulled <= self.order[way].index((piece, hop - 1)):
                    self.pull()
            for way in range(2):
                if self.pushed >= SLOTS:
                    self.copy(way, self.pushed - SLOTS).wait_send()
                self.copy(way, self.pushed).start()
            self.pushed += 1

    def pull(self):
        if self.pulled < self.total:
            for way in range(2):
                self.copy(way, self.pulled).wait_recv()
            self.pulled += 1

    def step(self, times=1):
        for _ in range(times):
            self.pull()
            self.push()

    def until(self, pulled):
        while self.pulled < pulled:
            self.step()

    def paced(self, index, counts):
        for i, times in enumerate(counts):
            if times:

                @pl.when(index == i)
                def _():
                    self.step(times)

    def drain(self):
        for step in range(max(self.total - SLOTS, 0), self.total):
            for way in range(2):
                self.copy(way, step).wait_send()


def greet(others):
    barrier = pltpu.get_barrier_semaphore()
    for other in others:
        pl.semaphore_signal(barrier, inc=1, device_id=other, device_id_type=MESH)
    pl.semaphore_wait(barrier, len(others))


def peers():
    tp = lax.axis_index("tp")
    chips = lax.axis_size("tp") // CORES
    chip, core = tp // CORES, tp % CORES
    partner = {"tp": chip * CORES + 1 - core}
    across = [{"tp": lax.rem(chip + s, chips) * CORES + core} for s in range(1, chips)]
    return chip, core, partner, across


def silu(x):
    return x / (1.0 + jnp.exp(-x))


def dot(a, b, dims=((1,), (0,)), precision=None):
    return lax.dot_general(
        a, b, (dims, ((), ())), precision=precision, preferred_element_type=jnp.float32
    )


def layer_kernel(
    arriving, content, leaving, pairs, gate_own, up_own, down_own, blend_hbm,
    raw, spike, value_taps, map_taps, shift, fading, skip, rescale, gain,
    out,
    padded, map_padded, regroup, leave, blend, arrived, entering, mixer, mixed, state,
    cums, steps, reach, prior,
    messages, chain, partial, from_partner, from_across, mid, resid,
    gate, up, hidden, down, made, made_partner, made_across,
    local_sem, halo_sem, ring_send, ring_recv, plane_send, plane_recv, chain_sem,
    core_sem, across_sem, mid_sem, made_core_sem, made_across_sem,
):
    length, channels = content.shape
    heads = raw.shape[0]
    size = channels // heads
    groups = map_taps.shape[1]
    wide = channels // groups
    per_group = heads // groups
    taps = value_taps.shape[0]
    kinds = groups * 2
    blocks = length // BLOCK
    half = length // CORES
    half_blocks = half // BLOCK
    count = lax.axis_size("sp")
    me = lax.axis_index("sp")
    tp = lax.axis_index("tp")
    per_tp = count // lax.axis_size("tp")
    chip, core, partner, across = peers()
    chips = len(across) + 1
    depth = gate_own.shape[0]
    planes, inner = ring_shape(count)
    plane, spoke = me // inner, lax.rem(me, inner)
    sides, units = down.shape[1], down.shape[2]

    loads = [
        pltpu.make_async_copy(content, padded.at[HALO:], local_sem.at[0]),
        pltpu.make_async_copy(pairs, map_padded.at[HALO * kinds :], local_sem.at[1]),
        pltpu.make_async_copy(leaving, leave, local_sem.at[2]),
        pltpu.make_async_copy(blend_hbm, blend, local_sem.at[3]),
        pltpu.make_async_copy(
            arriving.at[pl.ds(pl.multiple_of(core * half, half), half)], arrived, local_sem.at[4]
        ),
    ]
    mine = pl.ds(pl.multiple_of(me * depth, depth), depth)
    loads.append(pltpu.make_async_copy(gate_own, gate.at[mine], local_sem.at[5]))
    loads.append(pltpu.make_async_copy(up_own, up.at[mine], local_sem.at[6]))
    for side in range(sides):
        loads.append(
            pltpu.make_async_copy(
                down_own.at[:, pl.ds(side * BLOCK, BLOCK)], down.at[me, side], local_sem.at[7 + side]
            )
        )
    loads[0].start()
    loads[1].start()

    def rows_piece(own, whole, part):
        tall = depth // PIECES

        def refs(first, owner):
            at = pl.multiple_of(owner * depth + part * tall, tall)
            target = whole.at[pl.ds(at, tall)]
            return (own.at[pl.ds(part * tall, tall)] if first else target), target

        return refs

    def down_piece(side, part):
        rows = pl.ds(part * (units // 2), units // 2)

        def refs(first, owner):
            target = down.at[owner, side, rows]
            source = down_own.at[rows, pl.ds(side * BLOCK, BLOCK)]
            return (source if first else target), target

        return refs

    flow = Flow(
        [
            [rows_piece(gate_own, gate, part) for part in range(PIECES)]
            + [rows_piece(up_own, up, part) for part in range(PIECES)],
            [down_piece(side, part) for side in range(sides) for part in range(2)],
        ],
        ring_send,
        ring_recv,
    )
    fed = flow.ends[flow.hops - 1]
    before = {"sp": lax.rem(me + count - 1, count)}
    after = {"sp": lax.rem(me + 1, count)}
    siblings = [{"sp": plane * inner + lax.rem(spoke + s, inner)} for s in range(1, inner)]
    below = {"sp": lax.rem(me + inner, count)}
    above = {"sp": lax.rem(me + count - inner, count)}
    greet(
        [
            {"sp": flow.next[0]}, {"sp": flow.next[1]}, before, after, below, above,
            partner, *across, *siblings,
        ]
    )

    def halo(which, src, dst, rows):
        return pltpu.make_async_remote_copy(
            src_ref=src.at[src.shape[0] - rows :],
            dst_ref=dst.at[:rows],
            send_sem=halo_sem.at[which, 0],
            recv_sem=halo_sem.at[which, 1],
            device_id=after,
            device_id_type=MESH,
        )

    halos = [halo(0, content, padded, HALO), halo(1, pairs, map_padded, HALO * kinds)]

    @pl.when(me < count - 1)
    def _():
        for h in halos:
            h.start()

    for _ in range(DEPTH):
        flow.push()
    for load in loads[2:]:
        load.start()

    @pl.when(me == 0)
    def _():
        padded[:HALO] = jnp.zeros((HALO, channels), padded.dtype)
        map_padded[: HALO * kinds] = jnp.zeros((HALO * kinds, BLOCK), padded.dtype)

    to = lax.broadcasted_iota(jnp.int32, regroup.shape, 0)
    at = lax.broadcasted_iota(jnp.int32, regroup.shape, 1)
    regroup[...] = jnp.where(to == lax.rem(at, kinds) * BLOCK + at // kinds, 1.0, 0.0).astype(
        jnp.bfloat16
    )
    state[...] = jnp.zeros_like(state)
    prior[...] = jnp.zeros_like(prior)
    loads[0].wait()
    loads[1].wait()

    @pl.when(me > 0)
    def _():
        for h in halos:
            h.wait_recv()

    head = lax.broadcasted_iota(jnp.int32, (heads, channels), 0)
    place = lax.broadcasted_iota(jnp.int32, (heads, channels), 1) // size
    spread = jnp.where(head == place, 1.0, 0.0).astype(jnp.bfloat16)
    spread = jnp.concatenate([spread] * 3, axis=0)

    def expand(per_head):
        upper = per_head.astype(jnp.bfloat16)
        rest = per_head - upper.astype(jnp.float32)
        middle = rest.astype(jnp.bfloat16)
        lower = (rest - middle.astype(jnp.float32)).astype(jnp.bfloat16)
        return dot(jnp.concatenate([upper, middle, lower], axis=1), spread)

    def conv(ref, weights, start, first, width):
        x = ref[pl.ds(start, BLOCK + HALO), first : first + width].astype(jnp.float32)
        total = x[HALO:] * weights[taps - 1]
        for tap in range(taps - 1):
            total += pltpu.roll(x, taps - 1 - tap, 0)[HALO:] * weights[tap]
        return silu(total).astype(jnp.bfloat16)

    def map_conv(start):
        tall = BLOCK * kinds
        first = pl.multiple_of(start * kinds, tall)
        x = map_padded[pl.ds(first, tall + HALO * kinds), :].astype(jnp.float32)
        total = jnp.zeros((tall // 8, 8, BLOCK), jnp.float32)
        for tap in range(taps):
            line = [
                map_taps[tap, kind // 2, kind % 2 : kind % 2 + 1, :].astype(jnp.float32)
                for kind in range(kinds)
            ]
            weights = jnp.concatenate(line * (8 // kinds), axis=0)
            moved = x if tap == taps - 1 else pltpu.roll(x, (taps - 1 - tap) * kinds, 0)
            total += moved[HALO * kinds :].reshape(total.shape) * weights[None]
        maps = silu(total).reshape(tall, BLOCK).astype(jnp.bfloat16)
        return dot(regroup[...], maps).astype(jnp.bfloat16)

    row = lax.broadcasted_iota(jnp.int32, (BLOCK, BLOCK), 0)
    column = lax.broadcasted_iota(jnp.int32, (BLOCK, BLOCK), 1)
    causal = row >= column
    low = column < size
    running = jnp.where(row <= column, 1.0, 0.0)
    shift_rows = jnp.transpose(jnp.broadcast_to(shift[...], (BLOCK, heads)))
    rate_rows = jnp.transpose(jnp.broadcast_to(-jnp.exp(fading[...]), (BLOCK, heads)))
    direct = expand(jnp.broadcast_to(skip[...], (8, heads)))[0:1]

    def map_rows(start, kind):
        return pl.ds(pl.multiple_of(start * kinds, BLOCK) + kind * BLOCK, BLOCK)

    def state_step(block, _):
        start = pl.multiple_of(block * BLOCK, BLOCK)
        rows = pl.ds(start, BLOCK)
        raised = raw[:, rows].astype(jnp.float32) + shift_rows
        step_rows = jnp.maximum(raised, 0.0) + jnp.log1p(jnp.exp(-jnp.abs(raised)))
        log_decay = rate_rows * step_rows + spike[:, rows]
        cum_rows = dot(log_decay, running, precision=HIGHEST)
        end = cum_rows[:, BLOCK - 1 : BLOCK]
        cums[:, rows] = cum_rows
        steps[:, rows] = step_rows
        reach[:, rows] = jnp.exp(cum_rows + prior[...])
        prior[...] += jnp.broadcast_to(end, prior.shape)
        columns = jnp.transpose(
            jnp.concatenate([step_rows * jnp.exp(end - cum_rows), jnp.exp(cum_rows)], axis=0)
        )
        scale = expand(columns[:, :heads])
        keep = expand(columns[BLOCK - 8 :, heads:])[7:8]
        maps = map_conv(start)
        map_padded[pl.ds(pl.multiple_of(start * kinds, BLOCK), BLOCK * kinds), :] = maps
        entering[block] = state[...].astype(jnp.bfloat16)
        for group in range(groups):
            write = maps[2 * group * BLOCK : (2 * group + 1) * BLOCK]
            first = group * wide
            parts = []
            for place in range(first, first + wide, BLOCK):
                span = slice(place, place + BLOCK)
                weights = [
                    value_taps[tap : tap + 1, span].astype(jnp.float32) for tap in range(taps)
                ]
                value = conv(padded, weights, start, place, BLOCK)
                padded[rows, span] = value
                parts.append((value.astype(jnp.float32) * scale[:, span]).astype(jnp.bfloat16))
            span = slice(first, first + wide)
            added = dot(write, jnp.concatenate(parts, axis=1), ((0,), (0,)))
            state[:, span] = state[:, span] * keep[:, span] + added
        return 0

    def block_step(block, _):
        start = pl.multiple_of(block * BLOCK, BLOCK)
        rows = pl.ds(start, BLOCK)
        cum_rows = cums[:, rows]
        step_rows = steps[:, rows]
        columns = jnp.transpose(jnp.concatenate([cum_rows, jnp.exp(cum_rows)], axis=0))
        cum = columns[:, :heads]
        grow = expand(columns[:, heads:])
        for group in range(groups):
            write = map_padded[map_rows(start, 2 * group), :]
            read = map_padded[map_rows(start, 2 * group + 1), :]
            inter = dot(read, write, ((1,), (1,)))
            first = group * wide
            carried = dot(read, entering[block, :, first : first + wide])
            for pair in range(per_group // 2):
                place = first + pair * 2 * size
                span = slice(place, place + 2 * size)
                value = padded[rows, span]
                sides_ = []
                for side in range(2):
                    h = group * per_group + 2 * pair + side
                    gap = cum[:, h : h + 1] - cum_rows[h : h + 1, :]
                    sides_.append(
                        (
                            inter
                            * jnp.exp(jnp.where(causal, gap, -1e30))
                            * step_rows[h : h + 1, :]
                        ).astype(jnp.bfloat16)
                    )
                zero = jnp.zeros_like(value)
                stacked = jnp.concatenate(
                    [jnp.where(low, value, zero), jnp.where(low, zero, value)], axis=0
                )
                within = dot(jnp.concatenate(sides_, axis=1), stacked)
                local = slice(pair * 2 * size, (pair + 1) * 2 * size)
                mixer[rows, span] = (
                    within
                    + carried[:, local] * grow[:, span]
                    + direct[:, span] * value.astype(jnp.float32)
                )
        return 0

    def local_step(turn, _):
        lax.fori_loop(2 * turn, 2 * turn + 2, state_step, 0)
        flow.paced(turn, [0, 0, 0, 1])
        return 0

    lax.fori_loop(0, blocks // 2, local_step, 0)

    total = expand(jnp.transpose(prior[...]))[0:1]
    upper = total.astype(jnp.bfloat16)
    rest = total - upper.astype(jnp.float32)
    middle = rest.astype(jnp.bfloat16)
    lower = (rest - middle.astype(jnp.float32)).astype(jnp.bfloat16)
    messages[spoke, BLOCK:] = jnp.concatenate(
        [upper, middle, lower, jnp.zeros((HALO - 3, channels), jnp.bfloat16)], axis=0
    )
    messages[spoke, :BLOCK] = state[...].astype(jnp.bfloat16)

    def to_sibling(s):
        return pltpu.make_async_remote_copy(
            src_ref=messages.at[spoke],
            dst_ref=messages.at[spoke],
            send_sem=plane_send.at[s],
            recv_sem=plane_recv.at[inner - 2 - s],
            device_id=siblings[s],
            device_id_type=MESH,
        )

    for s in range(inner - 1):
        to_sibling(s).start()

    bands = 2
    band = channels // bands

    def pass_on(part):
        span = pl.ds(part * band, band)
        return pltpu.make_async_remote_copy(
            src_ref=chain.at[1, :, span],
            dst_ref=chain.at[0, :, span],
            send_sem=chain_sem.at[0, part],
            recv_sem=chain_sem.at[1, part],
            device_id=below,
            device_id_type=MESH,
        )

    def logs_of(other):
        terms = messages[other, BLOCK:].astype(jnp.float32)
        return terms[0:1] + terms[1:2] + terms[2:3]

    def plane_sum(part, behind):
        span = slice(part * band, (part + 1) * band)
        logs = [logs_of(other) for other in range(inner)]
        summed = jnp.zeros((BLOCK, band), jnp.float32)
        log = jnp.zeros((1, band), jnp.float32)
        for other in reversed(range(inner)):
            theirs = messages[other, :BLOCK, span].astype(jnp.float32) * jnp.exp(log)
            if behind:
                counts = jnp.full((1, band), other, jnp.int32) < spoke
                summed += jnp.where(counts, theirs, 0.0)
                log += jnp.where(counts, logs[other][:, span], 0.0)
            else:
                summed += theirs
                log += logs[other][:, span]
        return summed, jnp.exp(log)

    def begin_chain():
        for s in range(inner - 1):
            to_sibling(inner - 2 - s).wait_recv()

        @pl.when(plane == 0)
        def _():
            chain[0] = jnp.zeros((BLOCK, channels), jnp.bfloat16)
            for part in range(bands):
                chain[1, :, part * band : (part + 1) * band] = plane_sum(part, False)[0].astype(
                    jnp.bfloat16
                )
                pass_on(part).start()

    def join_chain(link):
        @pl.when(plane == link + 1)
        def _():
            for part in range(bands):
                span = slice(part * band, (part + 1) * band)
                pass_on(part).wait_recv()
                if link + 2 < planes:
                    summed, decay = plane_sum(part, False)
                    chain[1, :, span] = (
                        chain[0, :, span].astype(jnp.float32) * decay + summed
                    ).astype(jnp.bfloat16)
                    pass_on(part).start()

    turns = blocks // 2

    def scan_step(turn, _):
        lax.fori_loop(2 * turn, 2 * turn + 2, block_step, 0)
        flow.paced(turn, [1, 2] + [3] * (turns - 2))

        @pl.when(turn == 1)
        def _():
            begin_chain()

        for link in range(min(turns - 2, planes - 1)):

            @pl.when(turn == link + 2)
            def _():
                join_chain(link)

        return 0

    lax.fori_loop(0, turns, scan_step, 0)
    for link in range(turns - 2, planes - 1):
        flow.step(3)
        join_chain(link)

    for part in range(bands):
        span = slice(part * band, (part + 1) * band)
        summed, decay = plane_sum(part, True)
        state[:, span] = chain[0, :, span].astype(jnp.float32) * decay + summed

    loads[2].wait()
    loads[3].wait()
    blend_width = blend.shape[1]
    pace = 512 if blend_width % 512 == 0 else blend_width

    def project(side, j):
        turn = (core + 1 + side) % CORES
        start = pl.multiple_of(turn * half + j * BLOCK, BLOCK)
        rows = pl.ds(start, BLOCK)
        grow = expand(jnp.transpose(reach[:, rows]))
        for group in range(groups):
            span = slice(group * wide, (group + 1) * wide)
            read = map_padded[map_rows(start, 2 * group + 1), :]
            more = dot(read, state[:, span].astype(jnp.bfloat16)) * grow[:, span]
            gated = (mixer[rows, span] + more) * silu(leave[rows, span].astype(jnp.float32))
            mean = jnp.mean(gated * gated, axis=1, keepdims=True)
            mixed[:, span] = (gated * lax.rsqrt(mean + EPS) * rescale[:, span]).astype(jnp.bfloat16)
        for first in range(0, blend_width, pace):
            partial[side, j, :, first : first + pace] = dot(
                mixed[...], blend[:, first : first + pace]
            ).astype(jnp.bfloat16)

    def to_partner(j):
        return pltpu.make_async_remote_copy(
            src_ref=partial.at[0, j],
            dst_ref=from_partner.at[j],
            send_sem=core_sem.at[0, j],
            recv_sem=core_sem.at[1, j],
            device_id=partner,
            device_id_type=MESH,
        )

    def to_across(s, j):
        return pltpu.make_async_remote_copy(
            src_ref=partial.at[1, j],
            dst_ref=from_across.at[s, j],
            send_sem=across_sem.at[0, s, j],
            recv_sem=across_sem.at[1, s, j],
            device_id=across[s],
            device_id_type=MESH,
        )

    def mid_rows(j):
        return pl.ds(pl.multiple_of(core * half + j * BLOCK, BLOCK), BLOCK)

    def share_mid(j):
        return pltpu.make_async_remote_copy(
            src_ref=mid.at[mid_rows(j)],
            dst_ref=mid.at[mid_rows(j)],
            send_sem=mid_sem.at[0, j],
            recv_sem=mid_sem.at[1, j],
            device_id=partner,
            device_id_type=MESH,
        )

    def exchange_step(j, _):
        project(0, j)
        to_partner(j).start()
        flow.paced(j, [0, 1, 1, 1])
        project(1, j)
        to_partner(j).wait_recv()
        partial[1, j] = (
            partial[1, j].astype(jnp.float32) + from_partner[j].astype(jnp.float32)
        ).astype(jnp.bfloat16)
        for s in range(len(across)):
            to_across(s, j).start()
        return 0

    def collect_step(j, _):
        flow.paced(j, [1, 3, 3, 3])
        total = partial[1, j].astype(jnp.float32)
        for s in range(len(across)):
            to_across(s, j).wait_recv()
            total += from_across[s, j].astype(jnp.float32)
        own = arrived[pl.ds(pl.multiple_of(j * BLOCK, BLOCK), BLOCK)].astype(jnp.float32)
        mid[mid_rows(j)] = (own + total).astype(jnp.bfloat16)
        share_mid(j).start()
        return 0

    lax.fori_loop(0, half_blocks, exchange_step, 0)
    loads[4].wait()
    lax.fori_loop(0, half_blocks, collect_step, 0)
    for j in range(half_blocks):
        share_mid(j).wait_recv()
        share_mid(j).wait_send()
    own_width = resid.shape[1]

    def norm_step(block, _):
        rows = pl.ds(pl.multiple_of(block * BLOCK, BLOCK), BLOCK)
        resid[rows, :] = mid[rows, pl.ds(pl.multiple_of(tp * own_width, own_width), own_width)]
        x = mid[rows, :].astype(jnp.float32)
        mean = jnp.mean(x * x, axis=1, keepdims=True)
        mid[rows, :] = (x * lax.rsqrt(mean + EPS) * gain[...]).astype(jnp.bfloat16)
        return 0

    lax.fori_loop(0, blocks, norm_step, 0)
    for load in loads[5:]:
        load.wait()
    flow.until(fed)

    tall = 256
    tiles = length // tall

    def hidden_step(tile, _):
        rows = pl.ds(pl.multiple_of(tile * tall, tall), tall)
        x = mid[rows, :]
        hidden[rows, :] = (silu(dot(x, gate[...])) * dot(x, up[...])).astype(jnp.bfloat16)
        flow.paced(tile, [1, 1, 1, 1])
        return 0

    lax.fori_loop(0, tiles, hidden_step, 0)

    order = [(me, 0)]
    for hop in range(1, flow.hops + 1):
        order.append((flow.owner(0, hop), hop))
        if 2 * hop < count:
            order.append((flow.owner(1, hop), hop))

    def target(k):
        goal = order[k][0] // per_tp
        return goal // CORES, goal % CORES

    def slot(k):
        owner = order[k][0]
        return owner // (per_tp * CORES) * per_tp + lax.rem(owner, per_tp)

    long = length // PARTS
    units_of = [(side, part) for side in range(sides) for part in range(PARTS)]

    def over_cores(k, unit):
        return pltpu.make_async_remote_copy(
            src_ref=made.at[k, unit],
            dst_ref=made_partner.at[slot(k), unit],
            send_sem=made_core_sem.at[0, k, unit],
            recv_sem=made_core_sem.at[1, k, unit],
            device_id=partner,
            device_id_type=MESH,
        )

    def over_chips(k, unit, s, into):
        return pltpu.make_async_remote_copy(
            src_ref=made.at[k, unit],
            dst_ref=made_across.at[into, lax.rem(order[k][0], per_tp), unit],
            send_sem=made_across_sem.at[0, s, k, unit],
            recv_sem=made_across_sem.at[1, into, k, unit],
            device_id=across[s],
            device_id_type=MESH,
        )

    def make(k, unit):
        side, part = units_of[unit]
        for first in range(0, long, tall):
            rows = slice(part * long + first, part * long + first + tall)
            made[k, unit, first : first + tall, :] = dot(
                hidden[rows, :], down[order[k][0], side]
            ).astype(jnp.bfloat16)

        @pl.when(target(k)[1] != core)
        def _():
            over_cores(k, unit).start()

    def combine(k, unit):
        goal_chip, goal_core = target(k)

        @pl.when(goal_core == core)
        def _():
            over_cores(k, unit).wait_recv()
            made[k, unit] = (
                made[k, unit].astype(jnp.float32) + made_partner[slot(k), unit].astype(jnp.float32)
            ).astype(jnp.bfloat16)
            for s in range(chips - 1):

                @pl.when(goal_chip == lax.rem(chip + s + 1, chips))
                def _():
                    over_chips(k, unit, s, chips - 2 - s).start()

    def finish(k, unit):
        owner = order[k][0]
        side, part = units_of[unit]

        @pl.when(owner // per_tp == tp)
        def _():
            total = made[k, unit].astype(jnp.float32)
            for s in range(chips - 1):
                over_chips(k, unit, s, s).wait_recv()
                total += made_across[s, lax.rem(owner, per_tp), unit].astype(jnp.float32)
            at = (lax.rem(owner, per_tp) * sides + side) * BLOCK
            to = pl.ds(pl.multiple_of(at, BLOCK), BLOCK)
            rows = slice(part * long, (part + 1) * long)
            out[rows, to] = (resid[rows, to].astype(jnp.float32) + 0.5 * total).astype(jnp.bfloat16)

    made_units, summed_units, finished = [], 0, 0

    def sum_up_to(n):
        nonlocal summed_units
        while summed_units < n:
            combine(*made_units[summed_units])
            summed_units += 1

    def finish_up_to(n):
        nonlocal finished
        while finished < n:
            finish(*made_units[finished])
            finished += 1

    def handle(ks, side, lag):
        for k in ks:
            for part in range(PARTS):
                make(k, side * PARTS + part)
                made_units.append((k, side * PARTS + part))
                sum_up_to(len(made_units) - lag)

    lag = 3
    for side in range(sides):
        handle([0], side, lag)
    flow.step()
    for hop in range(1, flow.hops + 1):
        ks = [k for k in range(len(order)) if order[k][1] == hop]
        begin, end = flow.ends[flow.hops + hop - 2], flow.ends[flow.hops + hop - 1]
        old = len(made_units)
        for side in range(sides):
            flow.until(begin + (end - begin) * (side + 1) // sides)
            handle(ks, side, lag if hop < 3 else 2)
            if 2 * hop < flow.hops:
                flow.step()
            if hop > 1:
                sum_up_to(len(made_units))
        if hop < flow.hops:
            finish_up_to(old)
    finish_up_to(len(made_units))

    @pl.when(me < count - 1)
    def _():
        for h in halos:
            h.wait_send()

    for s in range(inner - 1):
        to_sibling(s).wait_send()

    @pl.when(plane < planes - 1)
    def _():
        for part in range(bands):
            pass_on(part).wait_send()

    for j in range(half_blocks):
        to_partner(j).wait_send()
        for s in range(len(across)):
            to_across(s, j).wait_send()
    flow.drain()
    for k in range(len(order)):
        goal_chip, goal_core = target(k)

        @pl.when(goal_core != core)
        def _():
            for unit in range(len(units_of)):
                over_cores(k, unit).wait_send()

        for s in range(chips - 1):

            @pl.when((goal_core == core) & (goal_chip == lax.rem(chip + s + 1, chips)))
            def _():
                for unit in range(len(units_of)):
                    over_chips(k, unit, s, chips - 2 - s).wait_send()


def shards(
    arriving, content, leaving, linked, raw, spike, value_taps, map_taps,
    shift, fading, skip, rescale, blend, gain, gate, up, down,
):
    length, channels = content.shape
    heads = raw.shape[1]
    groups, state_size = linked.shape[1], linked.shape[3]
    kinds = groups * 2
    width = arriving.shape[1]
    count = lax.axis_size("sp")
    inner = ring_shape(count)[1]
    tp_count = lax.axis_size("tp")
    chips = tp_count // CORES
    half = length // CORES
    half_blocks = half // BLOCK
    units, cut = down.shape
    sides = cut // BLOCK
    per_tp = count // tp_count
    subs = sides * PARTS
    anywhere = pl.BlockSpec(memory_space=pl.ANY)
    inside = pl.BlockSpec(memory_space=pltpu.VMEM)
    bf16, f32 = jnp.bfloat16, jnp.float32
    dma = pltpu.SemaphoreType.DMA
    return pl.pallas_call(
        layer_kernel,
        out_shape=pltpu.VMEM((length, width // tp_count), bf16),
        in_specs=[anywhere] * 8 + [inside] * 9,
        out_specs=inside,
        scratch_shapes=[
            pltpu.VMEM((HALO + length, channels), bf16),
            pltpu.VMEM(((HALO + length) * kinds, state_size), bf16),
            pltpu.VMEM((BLOCK * kinds, BLOCK * kinds), bf16),
            pltpu.VMEM((length, channels), bf16),
            pltpu.VMEM((channels, width), bf16),
            pltpu.VMEM((half, width), bf16),
            pltpu.VMEM((length // BLOCK, state_size, channels), bf16),
            pltpu.VMEM((length, channels), f32),
            pltpu.VMEM((BLOCK, channels), bf16),
            pltpu.VMEM((state_size, channels), f32),
            pltpu.VMEM((heads, length), f32),
            pltpu.VMEM((heads, length), f32),
            pltpu.VMEM((heads, length), f32),
            pltpu.VMEM((heads, BLOCK), f32),
            pltpu.VMEM((inner, state_size + HALO, channels), bf16),
            pltpu.VMEM((2, state_size, channels), bf16),
            pltpu.VMEM((CORES, half_blocks, BLOCK, width), bf16),
            pltpu.VMEM((half_blocks, BLOCK, width), bf16),
            pltpu.VMEM((chips - 1, half_blocks, BLOCK, width), bf16),
            pltpu.VMEM((length, width), bf16),
            pltpu.VMEM((length, width // tp_count), bf16),
            pltpu.VMEM((width, units), bf16),
            pltpu.VMEM((width, units), bf16),
            pltpu.VMEM((length, units), bf16),
            pltpu.VMEM((count, sides, units, BLOCK), bf16),
            pltpu.VMEM((count, subs, length // PARTS, BLOCK), bf16),
            pltpu.VMEM((chips * per_tp, subs, length // PARTS, BLOCK), bf16),
            pltpu.VMEM((chips - 1, per_tp, subs, length // PARTS, BLOCK), bf16),
            dma((7 + sides,)),
            dma((2, 2)),
            dma((2, SLOTS)),
            dma((2, SLOTS)),
            dma((max(inner - 1, 1),)),
            dma((max(inner - 1, 1),)),
            dma((2, 2)),
            dma((2, half_blocks)),
            dma((2, chips - 1, half_blocks)),
            dma((2, half_blocks)),
            dma((2, count, subs)),
            dma((2, chips - 1, count, subs)),
        ],
        compiler_params=pltpu.CompilerParams(
            collective_id=0, has_side_effects=True, vmem_limit_bytes=VMEM_BYTES
        ),
        name="layer",
    )(
        arriving, content, leaving, linked.reshape(length * kinds, state_size), gate, up, down, blend,
        raw.T, spike.T, value_taps, map_taps,
        shift[None], fading[None], skip[None], rescale[None], gain[None],
    )


def solution(mesh):
    placed = (
        P("sp", None),
        P("sp", "tp"),
        P("sp", "tp"),
        P("sp", "tp", None, None),
        P("sp", "tp"),
        P("sp", "tp"),
        P(None, "tp"),
        P(None, "tp", None, None),
        P("tp"),
        P("tp"),
        P("tp"),
        P("tp"),
        P("tp", None),
        P(),
        P("sp", "tp"),
        P("sp", "tp"),
        P("tp", "sp"),
    )
    return jax.shard_map(
        shards, mesh=mesh, in_specs=placed, out_specs=P("sp", "tp"), check_vma=False
    )
```

```python
import jax
import jax.numpy as jnp
from jax import lax
from jax.experimental import pallas as pl
from jax.experimental.pallas import tpu as pltpu
from jax.sharding import PartitionSpec as P

BLOCK = 128
CORES = 2
EPS = 1e-06
HALO = 16
HIGHEST = lax.Precision.HIGHEST
MESH = pl.DeviceIdType.MESH
VMEM_BYTES = 65_500_000


def ring_shape(count):
    inner = 1
    while inner * inner * 4 <= count:
        inner *= 2
    outer = count // inner
    if inner == 1 or outer % 2:
        return count, 1
    return outer, inner


def ring_at(spot, count):
    outer, inner = ring_shape(count)
    if inner == 1:
        return spot
    if inner == 2:
        late = spot // outer
        return (1 - late) * spot * 2 + late * (2 * (count - 1 - spot) + 1)
    late = jnp.minimum(spot // outer, 1)
    rest = (spot - outer) * late
    lap, step = rest // (inner - 1), rest % (inner - 1)
    odd = lap % 2
    column = (1 + step) * (1 - odd) + (inner - 1 - step) * odd
    return (1 - late) * spot * inner + late * ((outer - 1 - lap) * inner + column)


def ring_spot(index, count):
    outer, inner = ring_shape(count)
    if inner == 1:
        return index
    plane, column = index // inner, index % inner
    late = jnp.minimum(column, 1)
    lap = outer - 1 - plane
    odd = lap % 2
    step = (column - 1) * (1 - odd) + (inner - 1 - column) * odd
    return (1 - late) * plane + late * (outer + lap * (inner - 1) + step)


PIECES = 4
PARTS = 4
SLOTS = 8
DEPTH = 3


class Flow:
    def __init__(self, sets, send_sem, recv_sem):
        count = lax.axis_size("sp")
        spot = ring_spot(lax.axis_index("sp"), count)
        self.count, self.hops, self.spot = count, count // 2, spot
        self.send_sem, self.recv_sem = send_sem, recv_sem
        self.pieces = [piece for group in sets for piece in group]
        self.next = (
            ring_at(lax.rem(spot + 1, count), count),
            ring_at(lax.rem(spot + count - 1, count), count),
        )
        self.order, self.ends = ([], []), []
        first = 0
        for group in sets:
            for hop in range(1, self.hops + 1):
                for piece in range(first, first + len(group)):
                    for way in range(2):
                        if 2 * hop < count or piece % 2 == way:
                            self.order[way].append((piece, hop))
                self.ends.append(len(self.order[0]))
            first += len(group)
        self.total = len(self.order[0])
        self.pushed = self.pulled = 0

    def owner(self, way, hop):
        shift = self.count - hop if way == 0 else hop
        return ring_at(lax.rem(self.spot + shift, self.count), self.count)

    def copy(self, way, step):
        piece, hop = self.order[way][step]
        src, dst = self.pieces[piece](hop == 1, self.owner(way, hop - 1))
        return pltpu.make_async_remote_copy(
            src_ref=src,
            dst_ref=dst,
            send_sem=self.send_sem.at[way, step % SLOTS],
            recv_sem=self.recv_sem.at[way, step % SLOTS],
            device_id={"sp": self.next[way]},
            device_id_type=MESH,
        )

    def push(self):
        if self.pushed < self.total:
            for way in range(2):
                piece, hop = self.order[way][self.pushed]
                while hop > 1 and self.pulled <= self.order[way].index((piece, hop - 1)):
                    self.pull()
            for way in range(2):
                if self.pushed >= SLOTS:
                    self.copy(way, self.pushed - SLOTS).wait_send()
                self.copy(way, self.pushed).start()
            self.pushed += 1

    def pull(self):
        if self.pulled < self.total:
            for way in range(2):
                self.copy(way, self.pulled).wait_recv()
            self.pulled += 1

    def step(self, times=1):
        for _ in range(times):
            self.pull()
            self.push()

    def until(self, pulled):
        while self.pulled < pulled:
            self.step()

    def paced(self, index, counts):
        for i, times in enumerate(counts):
            if times:

                @pl.when(index == i)
                def _():
                    self.step(times)

    def drain(self):
        for step in range(max(self.total - SLOTS, 0), self.total):
            for way in range(2):
                self.copy(way, step).wait_send()


def greet(others):
    barrier = pltpu.get_barrier_semaphore()
    for other in others:
        pl.semaphore_signal(barrier, inc=1, device_id=other, device_id_type=MESH)
    pl.semaphore_wait(barrier, len(others))


def peers():
    tp = lax.axis_index("tp")
    chips = lax.axis_size("tp") // CORES
    chip, core = tp // CORES, tp % CORES
    partner = {"tp": chip * CORES + 1 - core}
    across = [{"tp": lax.rem(chip + s, chips) * CORES + core} for s in range(1, chips)]
    return chip, core, partner, across


def silu(x):
    return x / (1.0 + jnp.exp(-x))


def dot(a, b, dims=((1,), (0,)), precision=None):
    return lax.dot_general(
        a, b, (dims, ((), ())), precision=precision, preferred_element_type=jnp.float32
    )


def layer_kernel(
    arriving, content, leaving, pairs, gate_own, up_own, down_own, blend_hbm,
    raw_hbm, spike_hbm, value_taps_hbm, map_taps_hbm, shift_hbm, fading_hbm, skip_hbm,
    rescale_hbm, gain_hbm,
    out,
    padded, map_padded, regroup, leave, blend, arrived, entering, mixer, mixed, state,
    cums, steps, reach, prior,
    messages, chain, partial, from_partner, from_across, mid, resid,
    gate, up, hidden, down, made, made_partner, made_across,
    local_sem, halo_sem, ring_send, ring_recv, plane_send, plane_recv, chain_sem,
    core_sem, across_sem, mid_sem, made_core_send, made_core_recv, made_across_send,
    made_across_recv, small_sem, *small,
):
    raw, spike, value_taps, map_taps, shift, fading, skip, rescale, gain = small
    small_hbm = (
        raw_hbm, spike_hbm, value_taps_hbm, map_taps_hbm, shift_hbm, fading_hbm, skip_hbm,
        rescale_hbm, gain_hbm,
    )
    length, channels = content.shape
    heads = raw.shape[0]
    size = channels // heads
    groups = map_taps.shape[1]
    wide = channels // groups
    per_group = heads // groups
    taps = value_taps.shape[0]
    kinds = groups * 2
    blocks = length // BLOCK
    half = length // CORES
    half_blocks = half // BLOCK
    count = lax.axis_size("sp")
    me = lax.axis_index("sp")
    tp = lax.axis_index("tp")
    per_tp = count // lax.axis_size("tp")
    chip, core, partner, across = peers()
    chips = len(across) + 1
    depth = gate_own.shape[0]
    planes, inner = ring_shape(count)
    plane, spoke = me // inner, lax.rem(me, inner)
    sides, units = down.shape[1], down.shape[2]

    loads = [
        pltpu.make_async_copy(content, padded.at[HALO:], local_sem.at[0]),
        pltpu.make_async_copy(pairs, map_padded.at[HALO * kinds :], local_sem.at[1]),
        pltpu.make_async_copy(leaving, leave, local_sem.at[2]),
        pltpu.make_async_copy(blend_hbm, blend, local_sem.at[3]),
        pltpu.make_async_copy(
            arriving.at[pl.ds(pl.multiple_of(core * half, half), half)], arrived, local_sem.at[4]
        ),
    ]
    mine = pl.ds(pl.multiple_of(me * depth, depth), depth)
    loads.append(pltpu.make_async_copy(gate_own, gate.at[mine], local_sem.at[5]))
    loads.append(pltpu.make_async_copy(up_own, up.at[mine], local_sem.at[6]))
    for side in range(sides):
        loads.append(
            pltpu.make_async_copy(
                down_own.at[:, pl.ds(side * BLOCK, BLOCK)], down.at[me, side], local_sem.at[7 + side]
            )
        )
    small_loads = [
        pltpu.make_async_copy(src, dst, small_sem.at[i])
        for i, (src, dst) in enumerate(zip(small_hbm, small))
    ]
    loads[0].start()
    loads[1].start()
    for load in small_loads:
        load.start()

    def rows_piece(own, whole, part):
        tall = depth // PIECES

        def refs(first, owner):
            at = pl.multiple_of(owner * depth + part * tall, tall)
            target = whole.at[pl.ds(at, tall)]
            return (own.at[pl.ds(part * tall, tall)] if first else target), target

        return refs

    def down_piece(side, part):
        rows = pl.ds(part * (units // 2), units // 2)

        def refs(first, owner):
            target = down.at[owner, side, rows]
            source = down_own.at[rows, pl.ds(side * BLOCK, BLOCK)]
            return (source if first else target), target

        return refs

    flow = Flow(
        [
            [rows_piece(gate_own, gate, part) for part in range(PIECES)]
            + [rows_piece(up_own, up, part) for part in range(PIECES)],
            [down_piece(side, part) for side in range(sides) for part in range(2)],
        ],
        ring_send,
        ring_recv,
    )
    fed = flow.ends[flow.hops - 1]
    before = {"sp": lax.rem(me + count - 1, count)}
    after = {"sp": lax.rem(me + 1, count)}
    siblings = [{"sp": plane * inner + lax.rem(spoke + s, inner)} for s in range(1, inner)]
    below = {"sp": lax.rem(me + inner, count)}
    above = {"sp": lax.rem(me + count - inner, count)}
    greet(
        [
            {"sp": flow.next[0]}, {"sp": flow.next[1]}, before, after, below, above,
            partner, *across, *siblings,
        ]
    )

    def halo(which, src, dst, rows):
        return pltpu.make_async_remote_copy(
            src_ref=src.at[src.shape[0] - rows :],
            dst_ref=dst.at[:rows],
            send_sem=halo_sem.at[which, 0],
            recv_sem=halo_sem.at[which, 1],
            device_id=after,
            device_id_type=MESH,
        )

    halos = [halo(0, content, padded, HALO), halo(1, pairs, map_padded, HALO * kinds)]

    @pl.when(me < count - 1)
    def _():
        for h in halos:
            h.start()

    for _ in range(DEPTH):
        flow.push()
    for load in loads[2:]:
        load.start()

    @pl.when(me == 0)
    def _():
        padded[:HALO] = jnp.zeros((HALO, channels), padded.dtype)
        map_padded[: HALO * kinds] = jnp.zeros((HALO * kinds, BLOCK), padded.dtype)

    to = lax.broadcasted_iota(jnp.int32, regroup.shape, 0)
    at = lax.broadcasted_iota(jnp.int32, regroup.shape, 1)
    regroup[...] = jnp.where(to == lax.rem(at, kinds) * BLOCK + at // kinds, 1.0, 0.0).astype(
        jnp.bfloat16
    )
    state[...] = jnp.zeros_like(state)
    prior[...] = jnp.zeros_like(prior)
    loads[0].wait()
    loads[1].wait()
    for load in small_loads:
        load.wait()

    @pl.when(me > 0)
    def _():
        for h in halos:
            h.wait_recv()

    head = lax.broadcasted_iota(jnp.int32, (heads, channels), 0)
    place = lax.broadcasted_iota(jnp.int32, (heads, channels), 1) // size
    spread = jnp.where(head == place, 1.0, 0.0).astype(jnp.bfloat16)
    spread = jnp.concatenate([spread] * 3, axis=0)

    def expand(per_head):
        upper = per_head.astype(jnp.bfloat16)
        rest = per_head - upper.astype(jnp.float32)
        middle = rest.astype(jnp.bfloat16)
        lower = (rest - middle.astype(jnp.float32)).astype(jnp.bfloat16)
        return dot(jnp.concatenate([upper, middle, lower], axis=1), spread)

    def conv(ref, weights, start, first, width):
        x = ref[pl.ds(start, BLOCK + HALO), first : first + width].astype(jnp.float32)
        total = x[HALO:] * weights[taps - 1]
        for tap in range(taps - 1):
            total += pltpu.roll(x, taps - 1 - tap, 0)[HALO:] * weights[tap]
        return silu(total).astype(jnp.bfloat16)

    def map_conv(start):
        tall = BLOCK * kinds
        first = pl.multiple_of(start * kinds, tall)
        x = map_padded[pl.ds(first, tall + HALO * kinds), :].astype(jnp.float32)
        total = jnp.zeros((tall // 8, 8, BLOCK), jnp.float32)
        for tap in range(taps):
            line = [
                map_taps[tap, kind // 2, kind % 2 : kind % 2 + 1, :].astype(jnp.float32)
                for kind in range(kinds)
            ]
            weights = jnp.concatenate(line * (8 // kinds), axis=0)
            moved = x if tap == taps - 1 else pltpu.roll(x, (taps - 1 - tap) * kinds, 0)
            total += moved[HALO * kinds :].reshape(total.shape) * weights[None]
        maps = silu(total).reshape(tall, BLOCK).astype(jnp.bfloat16)
        return dot(regroup[...], maps).astype(jnp.bfloat16)

    row = lax.broadcasted_iota(jnp.int32, (BLOCK, BLOCK), 0)
    column = lax.broadcasted_iota(jnp.int32, (BLOCK, BLOCK), 1)
    causal = row >= column
    low = column < size
    running = jnp.where(row <= column, 1.0, 0.0)
    shift_rows = jnp.transpose(jnp.broadcast_to(shift[...], (BLOCK, heads)))
    rate_rows = jnp.transpose(jnp.broadcast_to(-jnp.exp(fading[...]), (BLOCK, heads)))
    direct = expand(jnp.broadcast_to(skip[...], (8, heads)))[0:1]

    def map_rows(start, kind):
        return pl.ds(pl.multiple_of(start * kinds, BLOCK) + kind * BLOCK, BLOCK)

    def state_step(block, _):
        start = pl.multiple_of(block * BLOCK, BLOCK)
        rows = pl.ds(start, BLOCK)
        raised = raw[:, rows].astype(jnp.float32) + shift_rows
        step_rows = jnp.maximum(raised, 0.0) + jnp.log1p(jnp.exp(-jnp.abs(raised)))
        log_decay = rate_rows * step_rows + spike[:, rows]
        cum_rows = dot(log_decay, running, precision=HIGHEST)
        end = cum_rows[:, BLOCK - 1 : BLOCK]
        cums[:, rows] = cum_rows
        steps[:, rows] = step_rows
        reach[:, rows] = jnp.exp(cum_rows + prior[...])
        prior[...] += jnp.broadcast_to(end, prior.shape)
        columns = jnp.transpose(
            jnp.concatenate([step_rows * jnp.exp(end - cum_rows), jnp.exp(cum_rows)], axis=0)
        )
        scale = expand(columns[:, :heads])
        keep = expand(columns[BLOCK - 8 :, heads:])[7:8]
        maps = map_conv(start)
        map_padded[pl.ds(pl.multiple_of(start * kinds, BLOCK), BLOCK * kinds), :] = maps
        entering[block] = state[...].astype(jnp.bfloat16)
        for group in range(groups):
            write = maps[2 * group * BLOCK : (2 * group + 1) * BLOCK]
            first = group * wide
            parts = []
            for place in range(first, first + wide, BLOCK):
                span = slice(place, place + BLOCK)
                weights = [
                    value_taps[tap : tap + 1, span].astype(jnp.float32) for tap in range(taps)
                ]
                value = conv(padded, weights, start, place, BLOCK)
                padded[rows, span] = value
                parts.append((value.astype(jnp.float32) * scale[:, span]).astype(jnp.bfloat16))
            span = slice(first, first + wide)
            added = dot(write, jnp.concatenate(parts, axis=1), ((0,), (0,)))
            state[:, span] = state[:, span] * keep[:, span] + added
        return 0

    def block_step(block, _):
        start = pl.multiple_of(block * BLOCK, BLOCK)
        rows = pl.ds(start, BLOCK)
        cum_rows = cums[:, rows]
        step_rows = steps[:, rows]
        columns = jnp.transpose(jnp.concatenate([cum_rows, jnp.exp(cum_rows)], axis=0))
        cum = columns[:, :heads]
        grow = expand(columns[:, heads:])
        for group in range(groups):
            write = map_padded[map_rows(start, 2 * group), :]
            read = map_padded[map_rows(start, 2 * group + 1), :]
            inter = dot(read, write, ((1,), (1,)))
            first = group * wide
            carried = dot(read, entering[block, :, first : first + wide])
            for pair in range(per_group // 2):
                place = first + pair * 2 * size
                span = slice(place, place + 2 * size)
                value = padded[rows, span]
                sides_ = []
                for side in range(2):
                    h = group * per_group + 2 * pair + side
                    gap = cum[:, h : h + 1] - cum_rows[h : h + 1, :]
                    sides_.append(
                        (
                            inter
                            * jnp.exp(jnp.where(causal, gap, -1e30))
                            * step_rows[h : h + 1, :]
                        ).astype(jnp.bfloat16)
                    )
                zero = jnp.zeros_like(value)
                stacked = jnp.concatenate(
                    [jnp.where(low, value, zero), jnp.where(low, zero, value)], axis=0
                )
                within = dot(jnp.concatenate(sides_, axis=1), stacked)
                local = slice(pair * 2 * size, (pair + 1) * 2 * size)
                mixer[rows, span] = (
                    within
                    + carried[:, local] * grow[:, span]
                    + direct[:, span] * value.astype(jnp.float32)
                )
        return 0

    def local_step(turn, _):
        lax.fori_loop(2 * turn, 2 * turn + 2, state_step, 0)
        flow.paced(turn, [0, 0, 0, 1])
        return 0

    lax.fori_loop(0, blocks // 2, local_step, 0)

    total = expand(jnp.transpose(prior[...]))[0:1]
    upper = total.astype(jnp.bfloat16)
    rest = total - upper.astype(jnp.float32)
    middle = rest.astype(jnp.bfloat16)
    lower = (rest - middle.astype(jnp.float32)).astype(jnp.bfloat16)
    messages[spoke, BLOCK:] = jnp.concatenate(
        [upper, middle, lower, jnp.zeros((HALO - 3, channels), jnp.bfloat16)], axis=0
    )
    messages[spoke, :BLOCK] = state[...].astype(jnp.bfloat16)

    def to_sibling(s):
        return pltpu.make_async_remote_copy(
            src_ref=messages.at[spoke],
            dst_ref=messages.at[spoke],
            send_sem=plane_send.at[s],
            recv_sem=plane_recv.at[inner - 2 - s],
            device_id=siblings[s],
            device_id_type=MESH,
        )

    for s in range(inner - 1):
        to_sibling(s).start()

    bands = 2
    band = channels // bands

    def pass_on(part):
        span = pl.ds(part * band, band)
        return pltpu.make_async_remote_copy(
            src_ref=chain.at[1, :, span],
            dst_ref=chain.at[0, :, span],
            send_sem=chain_sem.at[0, part],
            recv_sem=chain_sem.at[1, part],
            device_id=below,
            device_id_type=MESH,
        )

    def logs_of(other):
        terms = messages[other, BLOCK:].astype(jnp.float32)
        return terms[0:1] + terms[1:2] + terms[2:3]

    def plane_sum(part, behind):
        span = slice(part * band, (part + 1) * band)
        logs = [logs_of(other) for other in range(inner)]
        summed = jnp.zeros((BLOCK, band), jnp.float32)
        log = jnp.zeros((1, band), jnp.float32)
        for other in reversed(range(inner)):
            theirs = messages[other, :BLOCK, span].astype(jnp.float32) * jnp.exp(log)
            if behind:
                counts = jnp.full((1, band), other, jnp.int32) < spoke
                summed += jnp.where(counts, theirs, 0.0)
                log += jnp.where(counts, logs[other][:, span], 0.0)
            else:
                summed += theirs
                log += logs[other][:, span]
        return summed, jnp.exp(log)

    def begin_chain():
        for s in range(inner - 1):
            to_sibling(inner - 2 - s).wait_recv()

        @pl.when(plane == 0)
        def _():
            chain[0] = jnp.zeros((BLOCK, channels), jnp.bfloat16)
            for part in range(bands):
                chain[1, :, part * band : (part + 1) * band] = plane_sum(part, False)[0].astype(
                    jnp.bfloat16
                )
                pass_on(part).start()

    def join_chain(link):
        @pl.when(plane == link + 1)
        def _():
            for part in range(bands):
                span = slice(part * band, (part + 1) * band)
                pass_on(part).wait_recv()
                if link + 2 < planes:
                    summed, decay = plane_sum(part, False)
                    chain[1, :, span] = (
                        chain[0, :, span].astype(jnp.float32) * decay + summed
                    ).astype(jnp.bfloat16)
                    pass_on(part).start()

    turns = blocks // 2

    def scan_step(turn, _):
        lax.fori_loop(2 * turn, 2 * turn + 2, block_step, 0)
        flow.paced(turn, [1, 2] + [3] * (turns - 2))

        @pl.when(turn == 1)
        def _():
            begin_chain()

        for link in range(min(turns - 2, planes - 1)):

            @pl.when(turn == link + 2)
            def _():
                join_chain(link)

        return 0

    lax.fori_loop(0, turns, scan_step, 0)
    for link in range(turns - 2, planes - 1):
        flow.step(3)
        join_chain(link)

    for part in range(bands):
        span = slice(part * band, (part + 1) * band)
        summed, decay = plane_sum(part, True)
        state[:, span] = chain[0, :, span].astype(jnp.float32) * decay + summed

    loads[2].wait()
    loads[3].wait()
    blend_width = blend.shape[1]
    pace = 512 if blend_width % 512 == 0 else blend_width

    def project(side, j):
        turn = (core + 1 + side) % CORES
        start = pl.multiple_of(turn * half + j * BLOCK, BLOCK)
        rows = pl.ds(start, BLOCK)
        grow = expand(jnp.transpose(reach[:, rows]))
        for group in range(groups):
            span = slice(group * wide, (group + 1) * wide)
            read = map_padded[map_rows(start, 2 * group + 1), :]
            more = dot(read, state[:, span].astype(jnp.bfloat16)) * grow[:, span]
            gated = (mixer[rows, span] + more) * silu(leave[rows, span].astype(jnp.float32))
            mean = jnp.mean(gated * gated, axis=1, keepdims=True)
            mixed[:, span] = (gated * lax.rsqrt(mean + EPS) * rescale[:, span]).astype(jnp.bfloat16)
        for first in range(0, blend_width, pace):
            partial[side, j, :, first : first + pace] = dot(
                mixed[...], blend[:, first : first + pace]
            ).astype(jnp.bfloat16)

    def to_partner(j):
        return pltpu.make_async_remote_copy(
            src_ref=partial.at[0, j],
            dst_ref=from_partner.at[j],
            send_sem=core_sem.at[0, j],
            recv_sem=core_sem.at[1, j],
            device_id=partner,
            device_id_type=MESH,
        )

    def to_across(s, j):
        return pltpu.make_async_remote_copy(
            src_ref=partial.at[1, j],
            dst_ref=from_across.at[s, j],
            send_sem=across_sem.at[0, s, j],
            recv_sem=across_sem.at[1, s, j],
            device_id=across[s],
            device_id_type=MESH,
        )

    def mid_rows(j):
        return pl.ds(pl.multiple_of(core * half + j * BLOCK, BLOCK), BLOCK)

    def share_mid(j):
        return pltpu.make_async_remote_copy(
            src_ref=mid.at[mid_rows(j)],
            dst_ref=mid.at[mid_rows(j)],
            send_sem=mid_sem.at[0, j],
            recv_sem=mid_sem.at[1, j],
            device_id=partner,
            device_id_type=MESH,
        )

    def exchange_step(j, _):
        project(0, j)
        to_partner(j).start()
        flow.paced(j, [0, 1, 1, 1])
        project(1, j)
        to_partner(j).wait_recv()
        partial[1, j] = (
            partial[1, j].astype(jnp.float32) + from_partner[j].astype(jnp.float32)
        ).astype(jnp.bfloat16)
        for s in range(len(across)):
            to_across(s, j).start()
        return 0

    def collect_step(j, _):
        flow.paced(j, [1, 3, 3, 3])
        total = partial[1, j].astype(jnp.float32)
        for s in range(len(across)):
            to_across(s, j).wait_recv()
            total += from_across[s, j].astype(jnp.float32)
        own = arrived[pl.ds(pl.multiple_of(j * BLOCK, BLOCK), BLOCK)].astype(jnp.float32)
        mid[mid_rows(j)] = (own + total).astype(jnp.bfloat16)
        share_mid(j).start()
        return 0

    lax.fori_loop(0, half_blocks, exchange_step, 0)
    loads[4].wait()
    lax.fori_loop(0, half_blocks, collect_step, 0)
    for j in range(half_blocks):
        share_mid(j).wait_recv()
        share_mid(j).wait_send()
    own_width = resid.shape[1]

    def norm_step(block, _):
        rows = pl.ds(pl.multiple_of(block * BLOCK, BLOCK), BLOCK)
        resid[rows, :] = mid[rows, pl.ds(pl.multiple_of(tp * own_width, own_width), own_width)]
        x = mid[rows, :].astype(jnp.float32)
        mean = jnp.mean(x * x, axis=1, keepdims=True)
        mid[rows, :] = (x * lax.rsqrt(mean + EPS) * gain[...]).astype(jnp.bfloat16)
        return 0

    lax.fori_loop(0, blocks, norm_step, 0)
    for load in loads[5:]:
        load.wait()
    flow.until(fed)

    tall = 256
    tiles = length // tall

    def hidden_step(tile, _):
        rows = pl.ds(pl.multiple_of(tile * tall, tall), tall)
        x = mid[rows, :]
        hidden[rows, :] = (silu(dot(x, gate[...])) * dot(x, up[...])).astype(jnp.bfloat16)
        flow.paced(tile, [1, 1, 1, 1])
        return 0

    lax.fori_loop(0, tiles, hidden_step, 0)

    order = [(me, 0)]
    for hop in range(1, flow.hops + 1):
        order.append((flow.owner(0, hop), hop))
        if 2 * hop < count:
            order.append((flow.owner(1, hop), hop))

    def target(k):
        goal = order[k][0] // per_tp
        return goal // CORES, goal % CORES

    def slot(k):
        owner = order[k][0]
        return owner // (per_tp * CORES) * per_tp + lax.rem(owner, per_tp)

    long = length // PARTS
    units_of = [(side, part) for side in range(sides) for part in range(PARTS)]

    def over_cores(k, unit):
        return pltpu.make_async_remote_copy(
            src_ref=made.at[k, unit],
            dst_ref=made_partner.at[slot(k), unit],
            send_sem=made_core_send.at[0],
            recv_sem=made_core_recv.at[slot(k), unit],
            device_id=partner,
            device_id_type=MESH,
        )

    def over_chips(k, unit, s, into):
        return pltpu.make_async_remote_copy(
            src_ref=made.at[k, unit],
            dst_ref=made_across.at[into, lax.rem(order[k][0], per_tp), unit],
            send_sem=made_across_send.at[s],
            recv_sem=made_across_recv.at[into, lax.rem(order[k][0], per_tp), unit],
            device_id=across[s],
            device_id_type=MESH,
        )

    def make(k, unit):
        side, part = units_of[unit]
        for first in range(0, long, tall):
            rows = slice(part * long + first, part * long + first + tall)
            made[k, unit, first : first + tall, :] = dot(
                hidden[rows, :], down[order[k][0], side]
            ).astype(jnp.bfloat16)

        @pl.when(target(k)[1] != core)
        def _():
            over_cores(k, unit).start()

    def combine(k, unit):
        goal_chip, goal_core = target(k)

        @pl.when(goal_core == core)
        def _():
            over_cores(k, unit).wait_recv()
            made[k, unit] = (
                made[k, unit].astype(jnp.float32) + made_partner[slot(k), unit].astype(jnp.float32)
            ).astype(jnp.bfloat16)
            for s in range(chips - 1):

                @pl.when(goal_chip == lax.rem(chip + s + 1, chips))
                def _():
                    over_chips(k, unit, s, chips - 2 - s).start()

    def finish(k, unit):
        owner = order[k][0]
        side, part = units_of[unit]

        @pl.when(owner // per_tp == tp)
        def _():
            total = made[k, unit].astype(jnp.float32)
            for s in range(chips - 1):
                over_chips(k, unit, s, s).wait_recv()
                total += made_across[s, lax.rem(owner, per_tp), unit].astype(jnp.float32)
            at = (lax.rem(owner, per_tp) * sides + side) * BLOCK
            to = pl.ds(pl.multiple_of(at, BLOCK), BLOCK)
            rows = slice(part * long, (part + 1) * long)
            out[rows, to] = (resid[rows, to].astype(jnp.float32) + 0.5 * total).astype(jnp.bfloat16)

    made_units, summed_units, finished = [], 0, 0

    def sum_up_to(n):
        nonlocal summed_units
        while summed_units < n:
            combine(*made_units[summed_units])
            summed_units += 1

    def finish_up_to(n):
        nonlocal finished
        while finished < n:
            finish(*made_units[finished])
            finished += 1

    def handle(ks, side, lag):
        for k in ks:
            for part in range(PARTS):
                make(k, side * PARTS + part)
                made_units.append((k, side * PARTS + part))
                sum_up_to(len(made_units) - lag)

    lag = 3
    for side in range(sides):
        handle([0], side, lag)
    flow.step()
    for hop in range(1, flow.hops + 1):
        ks = [k for k in range(len(order)) if order[k][1] == hop]
        begin, end = flow.ends[flow.hops + hop - 2], flow.ends[flow.hops + hop - 1]
        old = len(made_units)
        for side in range(sides):
            flow.until(begin + (end - begin) * (side + 1) // sides)
            handle(ks, side, lag if hop < 3 else 2)
            if 2 * hop < flow.hops:
                flow.step()
            if hop > 1:
                sum_up_to(len(made_units))
        if hop < flow.hops:
            finish_up_to(old)
    finish_up_to(len(made_units))

    @pl.when(me < count - 1)
    def _():
        for h in halos:
            h.wait_send()

    for s in range(inner - 1):
        to_sibling(s).wait_send()

    @pl.when(plane < planes - 1)
    def _():
        for part in range(bands):
            pass_on(part).wait_send()

    for j in range(half_blocks):
        to_partner(j).wait_send()
        for s in range(len(across)):
            to_across(s, j).wait_send()
    flow.drain()
    pltpu.make_async_remote_copy(
        src_ref=made.at[: chips * per_tp],
        dst_ref=made_partner,
        send_sem=made_core_send.at[0],
        recv_sem=made_core_recv.at[0, 0],
        device_id=partner,
        device_id_type=MESH,
    ).wait_send()
    for s in range(chips - 1):
        pltpu.make_async_remote_copy(
            src_ref=made.at[:per_tp],
            dst_ref=made_across.at[s],
            send_sem=made_across_send.at[s],
            recv_sem=made_across_recv.at[s, 0, 0],
            device_id=across[s],
            device_id_type=MESH,
        ).wait_send()


def shards(
    arriving, content, leaving, linked, raw, spike, value_taps, map_taps,
    shift, fading, skip, rescale, blend, gain, gate, up, down,
):
    length, channels = content.shape
    heads = raw.shape[1]
    groups, state_size = linked.shape[1], linked.shape[3]
    kinds = groups * 2
    width = arriving.shape[1]
    count = lax.axis_size("sp")
    inner = ring_shape(count)[1]
    tp_count = lax.axis_size("tp")
    chips = tp_count // CORES
    half = length // CORES
    half_blocks = half // BLOCK
    units, cut = down.shape
    sides = cut // BLOCK
    per_tp = count // tp_count
    subs = sides * PARTS
    anywhere = pl.BlockSpec(memory_space=pl.ANY)
    inside = pl.BlockSpec(memory_space=pltpu.VMEM)
    bf16, f32 = jnp.bfloat16, jnp.float32
    dma = pltpu.SemaphoreType.DMA
    small = (
        raw.T, spike.T, value_taps, map_taps,
        shift[None], fading[None], skip[None], rescale[None], gain[None],
    )
    return pl.pallas_call(
        layer_kernel,
        out_shape=pltpu.VMEM((length, width // tp_count), bf16),
        in_specs=[anywhere] * (8 + len(small)),
        out_specs=inside,
        scratch_shapes=[
            pltpu.VMEM((HALO + length, channels), bf16),
            pltpu.VMEM(((HALO + length) * kinds, state_size), bf16),
            pltpu.VMEM((BLOCK * kinds, BLOCK * kinds), bf16),
            pltpu.VMEM((length, channels), bf16),
            pltpu.VMEM((channels, width), bf16),
            pltpu.VMEM((half, width), bf16),
            pltpu.VMEM((length // BLOCK, state_size, channels), bf16),
            pltpu.VMEM((length, channels), f32),
            pltpu.VMEM((BLOCK, channels), bf16),
            pltpu.VMEM((state_size, channels), f32),
            pltpu.VMEM((heads, length), f32),
            pltpu.VMEM((heads, length), f32),
            pltpu.VMEM((heads, length), f32),
            pltpu.VMEM((heads, BLOCK), f32),
            pltpu.VMEM((inner, state_size + HALO, channels), bf16),
            pltpu.VMEM((2, state_size, channels), bf16),
            pltpu.VMEM((CORES, half_blocks, BLOCK, width), bf16),
            pltpu.VMEM((half_blocks, BLOCK, width), bf16),
            pltpu.VMEM((chips - 1, half_blocks, BLOCK, width), bf16),
            pltpu.VMEM((length, width), bf16),
            pltpu.VMEM((length, width // tp_count), bf16),
            pltpu.VMEM((width, units), bf16),
            pltpu.VMEM((width, units), bf16),
            pltpu.VMEM((length, units), bf16),
            pltpu.VMEM((count, sides, units, BLOCK), bf16),
            pltpu.VMEM((count, subs, length // PARTS, BLOCK), bf16),
            pltpu.VMEM((chips * per_tp, subs, length // PARTS, BLOCK), bf16),
            pltpu.VMEM((chips - 1, per_tp, subs, length // PARTS, BLOCK), bf16),
            dma((7 + sides,)),
            dma((2, 2)),
            dma((2, SLOTS)),
            dma((2, SLOTS)),
            dma((max(inner - 1, 1),)),
            dma((max(inner - 1, 1),)),
            dma((2, 2)),
            dma((2, half_blocks)),
            dma((2, chips - 1, half_blocks)),
            dma((2, half_blocks)),
            dma((1,)),
            dma((chips * per_tp, subs)),
            dma((chips - 1,)),
            dma((chips - 1, per_tp, subs)),
            dma((len(small),)),
            *[pltpu.VMEM(x.shape, x.dtype) for x in small],
        ],
        compiler_params=pltpu.CompilerParams(
            collective_id=0, has_side_effects=True, vmem_limit_bytes=VMEM_BYTES
        ),
        name="layer",
    )(
        arriving, content, leaving, linked.reshape(length * kinds, state_size), gate, up, down, blend,
        *small,
    )


def solution(mesh):
    placed = (
        P("sp", None),
        P("sp", "tp"),
        P("sp", "tp"),
        P("sp", "tp", None, None),
        P("sp", "tp"),
        P("sp", "tp"),
        P(None, "tp"),
        P(None, "tp", None, None),
        P("tp"),
        P("tp"),
        P("tp"),
        P("tp"),
        P("tp", None),
        P(),
        P("sp", "tp"),
        P("sp", "tp"),
        P("tp", "sp"),
    )
    return jax.shard_map(
        shards, mesh=mesh, in_specs=placed, out_specs=P("sp", "tp"), check_vma=False
    )
```

```python
import jax
import jax.numpy as jnp
from jax import lax
from jax.experimental import pallas as pl
from jax.experimental.pallas import tpu as pltpu
from jax.sharding import PartitionSpec as P

BLOCK = 128
CORES = 2
EPS = 1e-06
HALO = 16
HIGHEST = lax.Precision.HIGHEST
MESH = pl.DeviceIdType.MESH
VMEM_BYTES = 65_500_000


def ring_shape(count):
    inner = 1
    while inner * inner * 4 <= count:
        inner *= 2
    outer = count // inner
    if inner == 1 or outer % 2:
        return count, 1
    return outer, inner


def ring_at(spot, count):
    outer, inner = ring_shape(count)
    if inner == 1:
        return spot
    if inner == 2:
        late = spot // outer
        return (1 - late) * spot * 2 + late * (2 * (count - 1 - spot) + 1)
    late = jnp.minimum(spot // outer, 1)
    rest = (spot - outer) * late
    lap, step = rest // (inner - 1), rest % (inner - 1)
    odd = lap % 2
    column = (1 + step) * (1 - odd) + (inner - 1 - step) * odd
    return (1 - late) * spot * inner + late * ((outer - 1 - lap) * inner + column)


def ring_spot(index, count):
    outer, inner = ring_shape(count)
    if inner == 1:
        return index
    plane, column = index // inner, index % inner
    late = jnp.minimum(column, 1)
    lap = outer - 1 - plane
    odd = lap % 2
    step = (column - 1) * (1 - odd) + (inner - 1 - column) * odd
    return (1 - late) * plane + late * (outer + lap * (inner - 1) + step)


PIECES = 4
PARTS = 4
SLOTS = 8
DEPTH = 3


class Flow:
    def __init__(self, sets, send_sem, recv_sem, pair_sem, partner):
        count = lax.axis_size("sp")
        spot = ring_spot(lax.axis_index("sp"), count)
        self.count, self.hops, self.spot = count, count // 2, spot
        self.send_sem, self.recv_sem = send_sem, recv_sem
        self.pair_sem, self.partner = pair_sem, partner
        self.pieces = [piece for group in sets for piece in group]
        self.next = (
            ring_at(lax.rem(spot + 1, count), count),
            ring_at(lax.rem(spot + count - 1, count), count),
        )
        self.order, self.ends = ([], []), []
        first = 0
        for group in sets:
            for hop in range(1, self.hops + 1):
                for piece in range(first, first + len(group)):
                    for way in range(2):
                        if 2 * hop < count or piece % 2 == way:
                            self.order[way].append((piece, hop))
                self.ends.append(len(self.order[0]))
            first += len(group)
        self.total = len(self.order[0])
        self.pushed = self.pulled = 0

    def owner(self, way, hop):
        shift = self.count - hop if way == 0 else hop
        return ring_at(lax.rem(self.spot + shift, self.count), self.count)

    def copy(self, way, step):
        piece, hop = self.order[way][step]
        src, dst = self.pieces[piece](hop == 1, self.owner(way, hop - 1))
        return pltpu.make_async_remote_copy(
            src_ref=src,
            dst_ref=dst,
            send_sem=self.send_sem.at[way, step % SLOTS],
            recv_sem=self.recv_sem.at[way, step % SLOTS],
            device_id={"sp": self.next[way]},
            device_id_type=MESH,
        )

    def push(self):
        if self.pushed < self.total:
            for way in range(2):
                piece, hop = self.order[way][self.pushed]
                while hop > 1 and self.pulled <= self.order[way].index((piece, hop - 1)):
                    self.pull()
            for way in range(2):
                if self.pushed >= SLOTS:
                    self.copy(way, self.pushed - SLOTS).wait_send()
                self.copy(way, self.pushed).start()
            self.pushed += 1

    def pull(self):
        if self.pulled < self.total:
            for way in range(2):
                self.copy(way, self.pulled).wait_recv()
            self.pulled += 1

    def step(self, times=1):
        for _ in range(times):
            self.pull()
            pl.semaphore_signal(
                self.pair_sem, inc=1, device_id=self.partner, device_id_type=MESH
            )
            pl.semaphore_wait(self.pair_sem, 1)
            self.push()

    def until(self, pulled):
        while self.pulled < pulled:
            self.step()

    def paced(self, index, counts):
        for i, times in enumerate(counts):
            if times:

                @pl.when(index == i)
                def _():
                    self.step(times)

    def drain(self):
        for step in range(max(self.total - SLOTS, 0), self.total):
            for way in range(2):
                self.copy(way, step).wait_send()


def greet(others):
    barrier = pltpu.get_barrier_semaphore()
    for other in others:
        pl.semaphore_signal(barrier, inc=1, device_id=other, device_id_type=MESH)
    pl.semaphore_wait(barrier, len(others))


def peers():
    tp = lax.axis_index("tp")
    chips = lax.axis_size("tp") // CORES
    chip, core = tp // CORES, tp % CORES
    partner = {"tp": chip * CORES + 1 - core}
    across = [{"tp": lax.rem(chip + s, chips) * CORES + core} for s in range(1, chips)]
    return chip, core, partner, across


def silu(x):
    return x / (1.0 + jnp.exp(-x))


def dot(a, b, dims=((1,), (0,)), precision=None):
    return lax.dot_general(
        a, b, (dims, ((), ())), precision=precision, preferred_element_type=jnp.float32
    )


def layer_kernel(
    arriving, content, leaving, pairs, gate_own, up_own, down_own, blend_hbm,
    raw_hbm, spike_hbm, value_taps_hbm, map_taps_hbm, shift_hbm, fading_hbm, skip_hbm,
    rescale_hbm, gain_hbm,
    out,
    padded, map_padded, regroup, leave, blend, arrived, entering, mixer, mixed, state,
    cums, steps, reach, prior,
    messages, chain, partial, from_partner, from_across, mid, resid,
    gate, up, hidden, down, made, made_partner, made_across,
    local_sem, halo_sem, ring_send, ring_recv, plane_send, plane_recv, chain_sem,
    core_sem, across_sem, mid_sem, made_core_send, made_core_recv, made_across_send,
    made_across_recv, pair_sem, small_sem, *small,
):
    raw, spike, value_taps, map_taps, shift, fading, skip, rescale, gain = small
    small_hbm = (
        raw_hbm, spike_hbm, value_taps_hbm, map_taps_hbm, shift_hbm, fading_hbm, skip_hbm,
        rescale_hbm, gain_hbm,
    )
    length, channels = content.shape
    heads = raw.shape[0]
    size = channels // heads
    groups = map_taps.shape[1]
    wide = channels // groups
    per_group = heads // groups
    taps = value_taps.shape[0]
    kinds = groups * 2
    blocks = length // BLOCK
    half = length // CORES
    half_blocks = half // BLOCK
    count = lax.axis_size("sp")
    me = lax.axis_index("sp")
    tp = lax.axis_index("tp")
    per_tp = count // lax.axis_size("tp")
    chip, core, partner, across = peers()
    chips = len(across) + 1
    depth = gate_own.shape[0]
    planes, inner = ring_shape(count)
    plane, spoke = me // inner, lax.rem(me, inner)
    sides, units = down.shape[1], down.shape[2]

    loads = [
        pltpu.make_async_copy(content, padded.at[HALO:], local_sem.at[0]),
        pltpu.make_async_copy(pairs, map_padded.at[HALO * kinds :], local_sem.at[1]),
        pltpu.make_async_copy(leaving, leave, local_sem.at[2]),
        pltpu.make_async_copy(blend_hbm, blend, local_sem.at[3]),
        pltpu.make_async_copy(
            arriving.at[pl.ds(pl.multiple_of(core * half, half), half)], arrived, local_sem.at[4]
        ),
    ]
    mine = pl.ds(pl.multiple_of(me * depth, depth), depth)
    loads.append(pltpu.make_async_copy(gate_own, gate.at[mine], local_sem.at[5]))
    loads.append(pltpu.make_async_copy(up_own, up.at[mine], local_sem.at[6]))
    for side in range(sides):
        loads.append(
            pltpu.make_async_copy(
                down_own.at[:, pl.ds(side * BLOCK, BLOCK)], down.at[me, side], local_sem.at[7 + side]
            )
        )
    small_loads = [
        pltpu.make_async_copy(src, dst, small_sem.at[i])
        for i, (src, dst) in enumerate(zip(small_hbm, small))
    ]
    loads[0].start()
    loads[1].start()
    for load in small_loads:
        load.start()

    def rows_piece(own, whole, part):
        tall = depth // PIECES

        def refs(first, owner):
            at = pl.multiple_of(owner * depth + part * tall, tall)
            target = whole.at[pl.ds(at, tall)]
            return (own.at[pl.ds(part * tall, tall)] if first else target), target

        return refs

    def down_piece(side, part):
        rows = pl.ds(part * (units // 2), units // 2)

        def refs(first, owner):
            target = down.at[owner, side, rows]
            source = down_own.at[rows, pl.ds(side * BLOCK, BLOCK)]
            return (source if first else target), target

        return refs

    flow = Flow(
        [
            [rows_piece(gate_own, gate, part) for part in range(PIECES)]
            + [rows_piece(up_own, up, part) for part in range(PIECES)],
            [down_piece(side, part) for side in range(sides) for part in range(2)],
        ],
        ring_send,
        ring_recv,
        pair_sem,
        partner,
    )
    fed = flow.ends[flow.hops - 1]
    before = {"sp": lax.rem(me + count - 1, count)}
    after = {"sp": lax.rem(me + 1, count)}
    siblings = [{"sp": plane * inner + lax.rem(spoke + s, inner)} for s in range(1, inner)]
    below = {"sp": lax.rem(me + inner, count)}
    above = {"sp": lax.rem(me + count - inner, count)}
    greet(
        [
            {"sp": flow.next[0]}, {"sp": flow.next[1]}, before, after, below, above,
            partner, *across, *siblings,
        ]
    )

    def halo(which, src, dst, rows):
        return pltpu.make_async_remote_copy(
            src_ref=src.at[src.shape[0] - rows :],
            dst_ref=dst.at[:rows],
            send_sem=halo_sem.at[which, 0],
            recv_sem=halo_sem.at[which, 1],
            device_id=after,
            device_id_type=MESH,
        )

    halos = [halo(0, content, padded, HALO), halo(1, pairs, map_padded, HALO * kinds)]

    @pl.when(me < count - 1)
    def _():
        for h in halos:
            h.start()

    for _ in range(DEPTH):
        flow.push()
    for load in loads[2:]:
        load.start()

    @pl.when(me == 0)
    def _():
        padded[:HALO] = jnp.zeros((HALO, channels), padded.dtype)
        map_padded[: HALO * kinds] = jnp.zeros((HALO * kinds, BLOCK), padded.dtype)

    to = lax.broadcasted_iota(jnp.int32, regroup.shape, 0)
    at = lax.broadcasted_iota(jnp.int32, regroup.shape, 1)
    regroup[...] = jnp.where(to == lax.rem(at, kinds) * BLOCK + at // kinds, 1.0, 0.0).astype(
        jnp.bfloat16
    )
    state[...] = jnp.zeros_like(state)
    prior[...] = jnp.zeros_like(prior)
    loads[0].wait()
    loads[1].wait()
    for load in small_loads:
        load.wait()

    @pl.when(me > 0)
    def _():
        for h in halos:
            h.wait_recv()

    head = lax.broadcasted_iota(jnp.int32, (heads, channels), 0)
    place = lax.broadcasted_iota(jnp.int32, (heads, channels), 1) // size
    spread = jnp.where(head == place, 1.0, 0.0).astype(jnp.bfloat16)
    spread = jnp.concatenate([spread] * 3, axis=0)

    def expand(per_head):
        upper = per_head.astype(jnp.bfloat16)
        rest = per_head - upper.astype(jnp.float32)
        middle = rest.astype(jnp.bfloat16)
        lower = (rest - middle.astype(jnp.float32)).astype(jnp.bfloat16)
        return dot(jnp.concatenate([upper, middle, lower], axis=1), spread)

    def conv(ref, weights, start, first, width):
        x = ref[pl.ds(start, BLOCK + HALO), first : first + width].astype(jnp.float32)
        total = x[HALO:] * weights[taps - 1]
        for tap in range(taps - 1):
            total += pltpu.roll(x, taps - 1 - tap, 0)[HALO:] * weights[tap]
        return silu(total).astype(jnp.bfloat16)

    def map_conv(start):
        tall = BLOCK * kinds
        first = pl.multiple_of(start * kinds, tall)
        x = map_padded[pl.ds(first, tall + HALO * kinds), :].astype(jnp.float32)
        total = jnp.zeros((tall // 8, 8, BLOCK), jnp.float32)
        for tap in range(taps):
            line = [
                map_taps[tap, kind // 2, kind % 2 : kind % 2 + 1, :].astype(jnp.float32)
                for kind in range(kinds)
            ]
            weights = jnp.concatenate(line * (8 // kinds), axis=0)
            moved = x if tap == taps - 1 else pltpu.roll(x, (taps - 1 - tap) * kinds, 0)
            total += moved[HALO * kinds :].reshape(total.shape) * weights[None]
        maps = silu(total).reshape(tall, BLOCK).astype(jnp.bfloat16)
        return dot(regroup[...], maps).astype(jnp.bfloat16)

    row = lax.broadcasted_iota(jnp.int32, (BLOCK, BLOCK), 0)
    column = lax.broadcasted_iota(jnp.int32, (BLOCK, BLOCK), 1)
    causal = row >= column
    low = column < size
    running = jnp.where(row <= column, 1.0, 0.0)
    shift_rows = jnp.transpose(jnp.broadcast_to(shift[...], (BLOCK, heads)))
    rate_rows = jnp.transpose(jnp.broadcast_to(-jnp.exp(fading[...]), (BLOCK, heads)))
    direct = expand(jnp.broadcast_to(skip[...], (8, heads)))[0:1]

    def map_rows(start, kind):
        return pl.ds(pl.multiple_of(start * kinds, BLOCK) + kind * BLOCK, BLOCK)

    def state_step(block, _):
        start = pl.multiple_of(block * BLOCK, BLOCK)
        rows = pl.ds(start, BLOCK)
        raised = raw[:, rows].astype(jnp.float32) + shift_rows
        step_rows = jnp.maximum(raised, 0.0) + jnp.log1p(jnp.exp(-jnp.abs(raised)))
        log_decay = rate_rows * step_rows + spike[:, rows]
        cum_rows = dot(log_decay, running, precision=HIGHEST)
        end = cum_rows[:, BLOCK - 1 : BLOCK]
        cums[:, rows] = cum_rows
        steps[:, rows] = step_rows
        reach[:, rows] = jnp.exp(cum_rows + prior[...])
        prior[...] += jnp.broadcast_to(end, prior.shape)
        columns = jnp.transpose(
            jnp.concatenate([step_rows * jnp.exp(end - cum_rows), jnp.exp(cum_rows)], axis=0)
        )
        scale = expand(columns[:, :heads])
        keep = expand(columns[BLOCK - 8 :, heads:])[7:8]
        maps = map_conv(start)
        map_padded[pl.ds(pl.multiple_of(start * kinds, BLOCK), BLOCK * kinds), :] = maps
        entering[block] = state[...].astype(jnp.bfloat16)
        for group in range(groups):
            write = maps[2 * group * BLOCK : (2 * group + 1) * BLOCK]
            first = group * wide
            parts = []
            for place in range(first, first + wide, BLOCK):
                span = slice(place, place + BLOCK)
                weights = [
                    value_taps[tap : tap + 1, span].astype(jnp.float32) for tap in range(taps)
                ]
                value = conv(padded, weights, start, place, BLOCK)
                padded[rows, span] = value
                parts.append((value.astype(jnp.float32) * scale[:, span]).astype(jnp.bfloat16))
            span = slice(first, first + wide)
            added = dot(write, jnp.concatenate(parts, axis=1), ((0,), (0,)))
            state[:, span] = state[:, span] * keep[:, span] + added
        return 0

    def block_step(block, _):
        start = pl.multiple_of(block * BLOCK, BLOCK)
        rows = pl.ds(start, BLOCK)
        cum_rows = cums[:, rows]
        step_rows = steps[:, rows]
        columns = jnp.transpose(jnp.concatenate([cum_rows, jnp.exp(cum_rows)], axis=0))
        cum = columns[:, :heads]
        grow = expand(columns[:, heads:])
        for group in range(groups):
            write = map_padded[map_rows(start, 2 * group), :]
            read = map_padded[map_rows(start, 2 * group + 1), :]
            inter = dot(read, write, ((1,), (1,)))
            first = group * wide
            carried = dot(read, entering[block, :, first : first + wide])
            for pair in range(per_group // 2):
                place = first + pair * 2 * size
                span = slice(place, place + 2 * size)
                value = padded[rows, span]
                sides_ = []
                for side in range(2):
                    h = group * per_group + 2 * pair + side
                    gap = cum[:, h : h + 1] - cum_rows[h : h + 1, :]
                    sides_.append(
                        (
                            inter
                            * jnp.exp(jnp.where(causal, gap, -1e30))
                            * step_rows[h : h + 1, :]
                        ).astype(jnp.bfloat16)
                    )
                zero = jnp.zeros_like(value)
                stacked = jnp.concatenate(
                    [jnp.where(low, value, zero), jnp.where(low, zero, value)], axis=0
                )
                within = dot(jnp.concatenate(sides_, axis=1), stacked)
                local = slice(pair * 2 * size, (pair + 1) * 2 * size)
                mixer[rows, span] = (
                    within
                    + carried[:, local] * grow[:, span]
                    + direct[:, span] * value.astype(jnp.float32)
                )
        return 0

    def local_step(turn, _):
        lax.fori_loop(2 * turn, 2 * turn + 2, state_step, 0)
        flow.paced(turn, [0, 0, 1, 1])
        return 0

    lax.fori_loop(0, blocks // 2, local_step, 0)

    total = expand(jnp.transpose(prior[...]))[0:1]
    upper = total.astype(jnp.bfloat16)
    rest = total - upper.astype(jnp.float32)
    middle = rest.astype(jnp.bfloat16)
    lower = (rest - middle.astype(jnp.float32)).astype(jnp.bfloat16)
    messages[spoke, BLOCK:] = jnp.concatenate(
        [upper, middle, lower, jnp.zeros((HALO - 3, channels), jnp.bfloat16)], axis=0
    )
    messages[spoke, :BLOCK] = state[...].astype(jnp.bfloat16)

    def to_sibling(s):
        return pltpu.make_async_remote_copy(
            src_ref=messages.at[spoke],
            dst_ref=messages.at[spoke],
            send_sem=plane_send.at[s],
            recv_sem=plane_recv.at[inner - 2 - s],
            device_id=siblings[s],
            device_id_type=MESH,
        )

    for s in range(inner - 1):
        to_sibling(s).start()

    bands = 2
    band = channels // bands

    def pass_on(part):
        span = pl.ds(part * band, band)
        return pltpu.make_async_remote_copy(
            src_ref=chain.at[1, :, span],
            dst_ref=chain.at[0, :, span],
            send_sem=chain_sem.at[0, part],
            recv_sem=chain_sem.at[1, part],
            device_id=below,
            device_id_type=MESH,
        )

    def logs_of(other):
        terms = messages[other, BLOCK:].astype(jnp.float32)
        return terms[0:1] + terms[1:2] + terms[2:3]

    def plane_sum(part, behind):
        span = slice(part * band, (part + 1) * band)
        logs = [logs_of(other) for other in range(inner)]
        summed = jnp.zeros((BLOCK, band), jnp.float32)
        log = jnp.zeros((1, band), jnp.float32)
        for other in reversed(range(inner)):
            theirs = messages[other, :BLOCK, span].astype(jnp.float32) * jnp.exp(log)
            if behind:
                counts = jnp.full((1, band), other, jnp.int32) < spoke
                summed += jnp.where(counts, theirs, 0.0)
                log += jnp.where(counts, logs[other][:, span], 0.0)
            else:
                summed += theirs
                log += logs[other][:, span]
        return summed, jnp.exp(log)

    def begin_chain():
        for s in range(inner - 1):
            to_sibling(inner - 2 - s).wait_recv()

        @pl.when(plane == 0)
        def _():
            chain[0] = jnp.zeros((BLOCK, channels), jnp.bfloat16)
            for part in range(bands):
                chain[1, :, part * band : (part + 1) * band] = plane_sum(part, False)[0].astype(
                    jnp.bfloat16
                )
                pass_on(part).start()

    def join_chain(link):
        @pl.when(plane == link + 1)
        def _():
            for part in range(bands):
                span = slice(part * band, (part + 1) * band)
                pass_on(part).wait_recv()
                if link + 2 < planes:
                    summed, decay = plane_sum(part, False)
                    chain[1, :, span] = (
                        chain[0, :, span].astype(jnp.float32) * decay + summed
                    ).astype(jnp.bfloat16)
                    pass_on(part).start()

    turns = blocks // 2

    def scan_step(turn, _):
        lax.fori_loop(2 * turn, 2 * turn + 2, block_step, 0)
        flow.paced(turn, [1, 2] + [3] * (turns - 2))

        @pl.when(turn == 1)
        def _():
            begin_chain()

        for link in range(min(turns - 2, planes - 1)):

            @pl.when(turn == link + 2)
            def _():
                join_chain(link)

        return 0

    lax.fori_loop(0, turns, scan_step, 0)
    for link in range(turns - 2, planes - 1):
        flow.step(3)
        join_chain(link)

    for part in range(bands):
        span = slice(part * band, (part + 1) * band)
        summed, decay = plane_sum(part, True)
        state[:, span] = chain[0, :, span].astype(jnp.float32) * decay + summed

    loads[2].wait()
    loads[3].wait()
    blend_width = blend.shape[1]
    pace = 512 if blend_width % 512 == 0 else blend_width

    def project(side, j):
        turn = (core + 1 + side) % CORES
        start = pl.multiple_of(turn * half + j * BLOCK, BLOCK)
        rows = pl.ds(start, BLOCK)
        grow = expand(jnp.transpose(reach[:, rows]))
        for group in range(groups):
            span = slice(group * wide, (group + 1) * wide)
            read = map_padded[map_rows(start, 2 * group + 1), :]
            more = dot(read, state[:, span].astype(jnp.bfloat16)) * grow[:, span]
            gated = (mixer[rows, span] + more) * silu(leave[rows, span].astype(jnp.float32))
            mean = jnp.mean(gated * gated, axis=1, keepdims=True)
            mixed[:, span] = (gated * lax.rsqrt(mean + EPS) * rescale[:, span]).astype(jnp.bfloat16)
        for first in range(0, blend_width, pace):
            partial[side, j, :, first : first + pace] = dot(
                mixed[...], blend[:, first : first + pace]
            ).astype(jnp.bfloat16)

    def to_partner(j):
        return pltpu.make_async_remote_copy(
            src_ref=partial.at[0, j],
            dst_ref=from_partner.at[j],
            send_sem=core_sem.at[0, j],
            recv_sem=core_sem.at[1, j],
            device_id=partner,
            device_id_type=MESH,
        )

    def to_across(s, j):
        return pltpu.make_async_remote_copy(
            src_ref=partial.at[1, j],
            dst_ref=from_across.at[s, j],
            send_sem=across_sem.at[0, s, j],
            recv_sem=across_sem.at[1, s, j],
            device_id=across[s],
            device_id_type=MESH,
        )

    def mid_rows(j):
        return pl.ds(pl.multiple_of(core * half + j * BLOCK, BLOCK), BLOCK)

    def share_mid(j):
        return pltpu.make_async_remote_copy(
            src_ref=mid.at[mid_rows(j)],
            dst_ref=mid.at[mid_rows(j)],
            send_sem=mid_sem.at[0, j],
            recv_sem=mid_sem.at[1, j],
            device_id=partner,
            device_id_type=MESH,
        )

    def exchange_step(j, _):
        project(0, j)
        to_partner(j).start()
        flow.paced(j, [0, 1, 1, 1])
        project(1, j)
        to_partner(j).wait_recv()
        partial[1, j] = (
            partial[1, j].astype(jnp.float32) + from_partner[j].astype(jnp.float32)
        ).astype(jnp.bfloat16)
        for s in range(len(across)):
            to_across(s, j).start()
        return 0

    def collect_step(j, _):
        flow.paced(j, [1, 3, 3, 3])
        total = partial[1, j].astype(jnp.float32)
        for s in range(len(across)):
            to_across(s, j).wait_recv()
            total += from_across[s, j].astype(jnp.float32)
        own = arrived[pl.ds(pl.multiple_of(j * BLOCK, BLOCK), BLOCK)].astype(jnp.float32)
        mid[mid_rows(j)] = (own + total).astype(jnp.bfloat16)
        share_mid(j).start()
        return 0

    lax.fori_loop(0, half_blocks, exchange_step, 0)
    loads[4].wait()
    lax.fori_loop(0, half_blocks, collect_step, 0)
    for j in range(half_blocks):
        share_mid(j).wait_recv()
        share_mid(j).wait_send()
    own_width = resid.shape[1]

    def norm_step(block, _):
        rows = pl.ds(pl.multiple_of(block * BLOCK, BLOCK), BLOCK)
        resid[rows, :] = mid[rows, pl.ds(pl.multiple_of(tp * own_width, own_width), own_width)]
        x = mid[rows, :].astype(jnp.float32)
        mean = jnp.mean(x * x, axis=1, keepdims=True)
        mid[rows, :] = (x * lax.rsqrt(mean + EPS) * gain[...]).astype(jnp.bfloat16)
        return 0

    lax.fori_loop(0, blocks, norm_step, 0)
    for load in loads[5:]:
        load.wait()
    flow.until(fed)

    tall = 256
    tiles = length // tall

    def hidden_step(tile, _):
        rows = pl.ds(pl.multiple_of(tile * tall, tall), tall)
        x = mid[rows, :]
        hidden[rows, :] = (silu(dot(x, gate[...])) * dot(x, up[...])).astype(jnp.bfloat16)
        flow.paced(tile, [1, 1, 1, 1])
        return 0

    lax.fori_loop(0, tiles, hidden_step, 0)

    order = [(me, 0)]
    for hop in range(1, flow.hops + 1):
        order.append((flow.owner(0, hop), hop))
        if 2 * hop < count:
            order.append((flow.owner(1, hop), hop))

    def target(k):
        goal = order[k][0] // per_tp
        return goal // CORES, goal % CORES

    def slot(k):
        owner = order[k][0]
        return owner // (per_tp * CORES) * per_tp + lax.rem(owner, per_tp)

    long = length // PARTS
    units_of = [(side, part) for side in range(sides) for part in range(PARTS)]

    def over_cores(k, unit):
        return pltpu.make_async_remote_copy(
            src_ref=made.at[k, unit],
            dst_ref=made_partner.at[slot(k), unit],
            send_sem=made_core_send.at[0],
            recv_sem=made_core_recv.at[slot(k), unit],
            device_id=partner,
            device_id_type=MESH,
        )

    def over_chips(k, unit, s, into):
        return pltpu.make_async_remote_copy(
            src_ref=made.at[k, unit],
            dst_ref=made_across.at[into, lax.rem(order[k][0], per_tp), unit],
            send_sem=made_across_send.at[s],
            recv_sem=made_across_recv.at[into, lax.rem(order[k][0], per_tp), unit],
            device_id=across[s],
            device_id_type=MESH,
        )

    def make(k, unit):
        side, part = units_of[unit]
        for first in range(0, long, tall):
            rows = slice(part * long + first, part * long + first + tall)
            made[k, unit, first : first + tall, :] = dot(
                hidden[rows, :], down[order[k][0], side]
            ).astype(jnp.bfloat16)

        @pl.when(target(k)[1] != core)
        def _():
            over_cores(k, unit).start()

    def combine(k, unit):
        goal_chip, goal_core = target(k)

        @pl.when(goal_core == core)
        def _():
            over_cores(k, unit).wait_recv()
            made[k, unit] = (
                made[k, unit].astype(jnp.float32) + made_partner[slot(k), unit].astype(jnp.float32)
            ).astype(jnp.bfloat16)
            for s in range(chips - 1):

                @pl.when(goal_chip == lax.rem(chip + s + 1, chips))
                def _():
                    over_chips(k, unit, s, chips - 2 - s).start()

    def finish(k, unit):
        owner = order[k][0]
        side, part = units_of[unit]

        @pl.when(owner // per_tp == tp)
        def _():
            total = made[k, unit].astype(jnp.float32)
            for s in range(chips - 1):
                over_chips(k, unit, s, s).wait_recv()
                total += made_across[s, lax.rem(owner, per_tp), unit].astype(jnp.float32)
            at = (lax.rem(owner, per_tp) * sides + side) * BLOCK
            to = pl.ds(pl.multiple_of(at, BLOCK), BLOCK)
            rows = slice(part * long, (part + 1) * long)
            out[rows, to] = (resid[rows, to].astype(jnp.float32) + 0.5 * total).astype(jnp.bfloat16)

    made_units, summed_units, finished = [], 0, 0

    def sum_up_to(n):
        nonlocal summed_units
        while summed_units < n:
            combine(*made_units[summed_units])
            summed_units += 1

    def finish_up_to(n):
        nonlocal finished
        while finished < n:
            finish(*made_units[finished])
            finished += 1

    def handle(ks, side, lag):
        for k in ks:
            for part in range(PARTS):
                make(k, side * PARTS + part)
                made_units.append((k, side * PARTS + part))
                sum_up_to(len(made_units) - lag)

    lag = 3
    for side in range(sides):
        handle([0], side, lag)
    flow.step()
    for hop in range(1, flow.hops + 1):
        ks = [k for k in range(len(order)) if order[k][1] == hop]
        begin, end = flow.ends[flow.hops + hop - 2], flow.ends[flow.hops + hop - 1]
        old = len(made_units)
        for side in range(sides):
            flow.until(begin + (end - begin) * (side + 1) // sides)
            handle(ks, side, lag if hop < 3 else 2)
            if 2 * hop < flow.hops:
                flow.step()
            if hop > 1:
                sum_up_to(len(made_units))
        if hop < flow.hops:
            finish_up_to(old)
    finish_up_to(len(made_units))

    @pl.when(me < count - 1)
    def _():
        for h in halos:
            h.wait_send()

    for s in range(inner - 1):
        to_sibling(s).wait_send()

    @pl.when(plane < planes - 1)
    def _():
        for part in range(bands):
            pass_on(part).wait_send()

    for j in range(half_blocks):
        to_partner(j).wait_send()
        for s in range(len(across)):
            to_across(s, j).wait_send()
    flow.drain()
    pltpu.make_async_remote_copy(
        src_ref=made.at[: chips * per_tp],
        dst_ref=made_partner,
        send_sem=made_core_send.at[0],
        recv_sem=made_core_recv.at[0, 0],
        device_id=partner,
        device_id_type=MESH,
    ).wait_send()
    for s in range(chips - 1):
        pltpu.make_async_remote_copy(
            src_ref=made.at[:per_tp],
            dst_ref=made_across.at[s],
            send_sem=made_across_send.at[s],
            recv_sem=made_across_recv.at[s, 0, 0],
            device_id=across[s],
            device_id_type=MESH,
        ).wait_send()


def shards(
    arriving, content, leaving, linked, raw, spike, value_taps, map_taps,
    shift, fading, skip, rescale, blend, gain, gate, up, down,
):
    length, channels = content.shape
    heads = raw.shape[1]
    groups, state_size = linked.shape[1], linked.shape[3]
    kinds = groups * 2
    width = arriving.shape[1]
    count = lax.axis_size("sp")
    inner = ring_shape(count)[1]
    tp_count = lax.axis_size("tp")
    chips = tp_count // CORES
    half = length // CORES
    half_blocks = half // BLOCK
    units, cut = down.shape
    sides = cut // BLOCK
    per_tp = count // tp_count
    subs = sides * PARTS
    anywhere = pl.BlockSpec(memory_space=pl.ANY)
    inside = pl.BlockSpec(memory_space=pltpu.VMEM)
    bf16, f32 = jnp.bfloat16, jnp.float32
    dma = pltpu.SemaphoreType.DMA
    small = (
        raw.T, spike.T, value_taps, map_taps,
        shift[None], fading[None], skip[None], rescale[None], gain[None],
    )
    return pl.pallas_call(
        layer_kernel,
        out_shape=pltpu.VMEM((length, width // tp_count), bf16),
        in_specs=[anywhere] * (8 + len(small)),
        out_specs=inside,
        scratch_shapes=[
            pltpu.VMEM((HALO + length, channels), bf16),
            pltpu.VMEM(((HALO + length) * kinds, state_size), bf16),
            pltpu.VMEM((BLOCK * kinds, BLOCK * kinds), bf16),
            pltpu.VMEM((length, channels), bf16),
            pltpu.VMEM((channels, width), bf16),
            pltpu.VMEM((half, width), bf16),
            pltpu.VMEM((length // BLOCK, state_size, channels), bf16),
            pltpu.VMEM((length, channels), f32),
            pltpu.VMEM((BLOCK, channels), bf16),
            pltpu.VMEM((state_size, channels), f32),
            pltpu.VMEM((heads, length), f32),
            pltpu.VMEM((heads, length), f32),
            pltpu.VMEM((heads, length), f32),
            pltpu.VMEM((heads, BLOCK), f32),
            pltpu.VMEM((inner, state_size + HALO, channels), bf16),
            pltpu.VMEM((2, state_size, channels), bf16),
            pltpu.VMEM((CORES, half_blocks, BLOCK, width), bf16),
            pltpu.VMEM((half_blocks, BLOCK, width), bf16),
            pltpu.VMEM((chips - 1, half_blocks, BLOCK, width), bf16),
            pltpu.VMEM((length, width), bf16),
            pltpu.VMEM((length, width // tp_count), bf16),
            pltpu.VMEM((width, units), bf16),
            pltpu.VMEM((width, units), bf16),
            pltpu.VMEM((length, units), bf16),
            pltpu.VMEM((count, sides, units, BLOCK), bf16),
            pltpu.VMEM((count, subs, length // PARTS, BLOCK), bf16),
            pltpu.VMEM((chips * per_tp, subs, length // PARTS, BLOCK), bf16),
            pltpu.VMEM((chips - 1, per_tp, subs, length // PARTS, BLOCK), bf16),
            dma((7 + sides,)),
            dma((2, 2)),
            dma((2, SLOTS)),
            dma((2, SLOTS)),
            dma((max(inner - 1, 1),)),
            dma((max(inner - 1, 1),)),
            dma((2, 2)),
            dma((2, half_blocks)),
            dma((2, chips - 1, half_blocks)),
            dma((2, half_blocks)),
            dma((1,)),
            dma((chips * per_tp, subs)),
            dma((chips - 1,)),
            dma((chips - 1, per_tp, subs)),
            pltpu.SemaphoreType.REGULAR,
            dma((len(small),)),
            *[pltpu.VMEM(x.shape, x.dtype) for x in small],
        ],
        compiler_params=pltpu.CompilerParams(
            collective_id=0, has_side_effects=True, vmem_limit_bytes=VMEM_BYTES
        ),
        name="layer",
    )(
        arriving, content, leaving, linked.reshape(length * kinds, state_size), gate, up, down, blend,
        *small,
    )


def solution(mesh):
    placed = (
        P("sp", None),
        P("sp", "tp"),
        P("sp", "tp"),
        P("sp", "tp", None, None),
        P("sp", "tp"),
        P("sp", "tp"),
        P(None, "tp"),
        P(None, "tp", None, None),
        P("tp"),
        P("tp"),
        P("tp"),
        P("tp"),
        P("tp", None),
        P(),
        P("sp", "tp"),
        P("sp", "tp"),
        P("tp", "sp"),
    )
    return jax.shard_map(
        shards, mesh=mesh, in_specs=placed, out_specs=P("sp", "tp"), check_vma=False
    )
```
